32 devices in a mesh: sp: 16 (over z, y, x), tp: 2 (over core).
Axes of the slice: x: 2, y: 2, z: 4, core: 2. Of those that a mesh axis runs over, the one named last changes fastest.
Arguments:
- queries_narrow: bfloat16 [4096, 1024], P('sp', 'tp'), may hold values from -40 to 40
- keys_narrow: bfloat16 [4096, 256], P('sp', 'tp'), may hold values from -40 to 40
- values_narrow: bfloat16 [4096, 256], P('sp', 'tp'), may hold values from -6 to 6
- queries_wide: bfloat16 [4096, 1024], P('sp', 'tp'), may hold values from -40 to 40
- keys_wide: bfloat16 [4096, 512], P('sp', 'tp'), may hold values from -40 to 40
- values_wide: bfloat16 [4096, 512], P('sp', 'tp'), may hold values from -6 to 6
- lambda_narrow: float32 [8], P('tp'), may hold values from 0.3 to 0.8
- lambda_wide: float32 [4], P('tp'), may hold values from 0.3 to 0.8
- gain_narrow: float32 [128], replicated, may hold values from 0.1 to 1.9
- gain_wide: float32 [256], replicated, may hold values from 0.1 to 1.9
- out_narrow: bfloat16 [1024, 2048], replicated, may hold values from -0.125 to 0.125
- out_wide: bfloat16 [1024, 2048], replicated, may hold values from -0.125 to 0.125
- stream: bfloat16 [4096, 2048], P(('sp', 'tp')), may hold values from -6 to 6
- gain_mix: float32 [2048], replicated, may hold values from 0.1 to 1.9
- gain_ffn: float32 [2048], replicated, may hold values from 0.1 to 1.9
- gain_post: float32 [2048], replicated, may hold values from 0.1 to 1.9
- shared_gate: bfloat16 [2048, 512], replicated, may hold values from -0.125 to 0.125
- shared_up: bfloat16 [2048, 512], replicated, may hold values from -0.125 to 0.125
- shared_down: bfloat16 [512, 2048], replicated, may hold values from -0.25 to 0.25
- expert_gate: bfloat16 [32, 2048, 512], P('sp', None, 'tp'), may hold values from -0.125 to 0.125
- expert_up: bfloat16 [32, 2048, 512], P('sp', None, 'tp'), may hold values from -0.125 to 0.125
- expert_down: bfloat16 [32, 512, 2048], P('sp', 'tp'), may hold values from -0.25 to 0.25
- expert_ids: int32 [4096, 4], P(('sp', 'tp')), may hold values from 0 to 31, all different within a row; in each aligned block of 128 rows (0 to 127, 128 to 255, ...) at most 24 rows name the same one
- route_weights: float32 [4096, 4], P(('sp', 'tp')), may hold values from 0.2 to 1
Outputs:
- layer_out: bfloat16 [4096, 2048], P(('sp', 'tp'))
The draws below stay inside these ranges and needn't reach their ends.
Inputs may be any that keep to these rules, and one draw needn't show every extreme that they name: `expert_ids`: the experts of one token differ. Within the rows that one device holds (aligned blocks of rows in the placement's order), no expert is named more than 24 times, and in every draw some expert is named exactly 24 times there.
All inputs are finite; a program needn't handle non-finite values.
Results may differ from the reference program's by a relative error of at most 0.015.
Values may be sent and summed in bfloat16 or wider, within the bound.
A program may use at most 192 MiB of HBM per device.

```python
import math
import jax
import jax.numpy as jnp
import numpy as np
from jax import lax

D = 2048
HN = 8
DN = 64
VN = 128
KN = 2
HW = 4
DW = 128
VW = 256
KW = 2
FF = 512
SFF = 512
TOPK = 4
TOK_DEV = 256
TOKENS = 4096
EXPERTS = 32
CAP = 24
N_SP = 16
N_TP = 2


def pair_draw(key, heads, groups, key_dim, salt):
    base = jax.random.fold_in(key, salt)
    query_key, keys_key = jax.random.split(base, 2)
    queries = jax.random.normal(query_key, (TOKENS, heads, 2, key_dim), jnp.float32) * 1.4
    keys = jax.random.normal(keys_key, (TOKENS, groups, 2, key_dim), jnp.float32) * 1.3
    queries = jnp.clip(queries, -40.0, 40.0)
    keys = jnp.clip(keys, -40.0, 40.0)
    return (queries.reshape(TOKENS, heads * 2 * key_dim), keys.reshape(TOKENS, groups * 2 * key_dim))


def draw_queries_narrow(key, part):
    return pair_draw(key, HN, KN, DN, 11)[0].astype(jnp.bfloat16)


def draw_keys_narrow(key, part):
    return pair_draw(key, HN, KN, DN, 11)[1].astype(jnp.bfloat16)


def draw_queries_wide(key, part):
    return pair_draw(key, HW, KW, DW, 12)[0].astype(jnp.bfloat16)


def draw_keys_wide(key, part):
    return pair_draw(key, HW, KW, DW, 12)[1].astype(jnp.bfloat16)


def block_levels(rng, dims, pieces, low, high):
    gain, own = 1.0, jax.random.fold_in(rng, 6)
    for axis_at, shards_of in pieces:
        draws = jnp.exp(jax.random.uniform(jax.random.fold_in(own, axis_at), (shards_of,), jnp.float32, low / len(pieces), high / len(pieces)))
        gain = gain * jnp.repeat(draws, dims[axis_at] // shards_of).reshape([-1 if axis == axis_at else 1 for axis in range(len(dims))])
    return gain


def routed_block(rng, own, number, rows, amount, top, bound, slope):
    order = jax.random.permutation(rng, amount)
    crowded, usual = load_shares(amount, rows * top, bound, slope, True), load_shares(amount, rows * top, bound, slope, False)
    places = jnp.arange(amount)

    def named(tallies, rotation):
        used = int((tallies > 0).sum())
        fixed = max(1, used // 4)
        moved = fixed + (places - fixed + rotation * (used - fixed)) % max(1, amount - fixed)
        return jnp.zeros((amount,), jnp.int32).at[order[jnp.where(places < fixed, places, moved)]].set(jnp.asarray(tallies, jnp.int32))

    tallies = jnp.where(number % 4 == 0, named(crowded, number // 4), named(usual, number - number // 4 - 1))
    mixed = jax.random.permutation(jax.random.fold_in(own, 3), amount)
    source_of, sink = mixed[0:amount // 2 * 2:2], mixed[1:amount // 2 * 2:2]
    room = jnp.minimum(tallies[source_of] - 1, bound - tallies[sink]) // 2
    room = jnp.where((source_of == order[0]) | (sink == order[0]) | (tallies[sink] == 0), 0, jnp.maximum(room, 0))
    moved = jax.random.randint(jax.random.fold_in(own, 4), (amount // 2,), 0, 1 << 20) % (room + 1)
    tallies = tallies.at[source_of].add(-moved).at[sink].add(moved)
    items = jnp.searchsorted(jnp.cumsum(tallies), jnp.arange(rows * top), side="right").astype(jnp.int32)
    listing = items.reshape(top, rows).T
    listing = listing[jax.random.permutation(jax.random.fold_in(own, 1), rows)]
    rotation = jax.random.randint(jax.random.fold_in(own, 2), (rows, 1), 0, top)
    return jnp.take_along_axis(listing, (jnp.arange(top)[None, :] + rotation) % top, axis=1)


def load_shares(count, total, reach, lean, full):
    loads = [(1 << 20) // math.isqrt(rank ** lean) + 1 for rank in range(1, count + 1)]
    largest = reach if full else min(reach, max(-(-total // count), total * loads[0] // sum(loads)))
    least = 1 if total - largest >= count - 1 else 0
    given, rest = [largest] + [least] * (count - 1), total - largest - least * (count - 1)
    while rest > 0:
        movable = [i for i in range(1, count) if given[i] < largest] or [i for i in range(1, count) if given[i] < reach]
        whole, budget = sum([loads[i] for i in movable]), rest
        for i in movable:
            extra = min(reach - given[i], max(1, budget * loads[i] // whole), rest)
            given[i] = given[i] + extra
            rest = rest - extra
    return np.array(given)


def normal_values(key, extent, scale, limit, shards=(), kind=jnp.bfloat16):
    values = scale * jax.random.normal(key, extent, jnp.float32)
    if shards:
        values = values * block_levels(key, extent, shards, -0.22, 0.18)
    return jnp.clip(values, -limit, limit).astype(kind)


def setup_inputs(seed: int = 0) -> dict:
    key_list = jax.random.split(jax.random.key(seed), 25)
    queries_narrow = draw_queries_narrow(jax.random.fold_in(key_list[24], 71), 0)
    keys_narrow = draw_keys_narrow(jax.random.fold_in(key_list[24], 71), 0)
    values_narrow = normal_values(key_list[2], (TOKENS, KN * VN), 1.0, 6.0, ((0, 16), (1, 2)))
    queries_wide = draw_queries_wide(jax.random.fold_in(key_list[24], 71), 0)
    keys_wide = draw_keys_wide(jax.random.fold_in(key_list[24], 71), 0)
    values_wide = normal_values(key_list[5], (TOKENS, KW * VW), 1.0, 6.0, ((0, 16), (1, 2)))
    lambda_narrow = jnp.clip(0.3 + 0.5 * jax.random.uniform(key_list[6], (HN,), jnp.float32) ** block_levels(key_list[6], (HN,), ((0, 2),), -0.2, 0.2), 0.3, 0.8)
    lambda_wide = jnp.clip(0.3 + 0.5 * jax.random.uniform(key_list[7], (HW,), jnp.float32) ** block_levels(key_list[7], (HW,), ((0, 2),), -0.2, 0.2), 0.3, 0.8)
    gain_narrow = jnp.clip(1.0 + 0.18 * jax.random.normal(key_list[8], (VN,), jnp.float32), 0.1, 1.9)
    gain_wide = jnp.clip(1.0 + 0.18 * jax.random.normal(key_list[9], (VW,), jnp.float32), 0.1, 1.9)
    out_narrow = normal_values(key_list[10], (HN * VN, D), D ** -0.5, 0.125)
    out_wide = normal_values(key_list[11], (HW * VW, D), D ** -0.5, 0.125)
    stream = normal_values(key_list[12], (TOKENS, D), 1.0, 6.0, ((0, 32),))
    gain_mix = jnp.clip(1.0 + 0.18 * jax.random.normal(key_list[13], (D,), jnp.float32), 0.1, 1.9)
    gain_ffn = jnp.clip(1.0 + 0.18 * jax.random.normal(key_list[14], (D,), jnp.float32), 0.1, 1.9)
    gain_post = jnp.clip(1.0 + 0.18 * jax.random.normal(key_list[15], (D,), jnp.float32), 0.1, 1.9)
    shared_gate = normal_values(key_list[16], (D, SFF), D ** -0.5, 0.125)
    shared_up = normal_values(key_list[17], (D, SFF), D ** -0.5, 0.125)
    shared_down = normal_values(key_list[18], (SFF, D), SFF ** -0.5, 0.25)
    expert_gate = normal_values(key_list[19], (EXPERTS, D, FF), D ** -0.5, 0.125, ((0, 16), (2, 2)))
    expert_up = normal_values(key_list[20], (EXPERTS, D, FF), D ** -0.5, 0.125, ((0, 16), (2, 2)))
    expert_down = normal_values(key_list[21], (EXPERTS, FF, D), FF ** -0.5, 0.25, ((0, 16), (1, 2)))
    expert_ids_keys = jax.random.split(jax.random.fold_in(key_list[22], 1), TOKENS // (TOK_DEV // N_TP))
    expert_ids_turns = jax.random.permutation(jax.random.fold_in(key_list[22], 3), TOKENS // (TOK_DEV // N_TP))
    expert_ids = jax.vmap(lambda own, number: routed_block(jax.random.fold_in(key_list[22], 2), own, number, TOK_DEV // N_TP, EXPERTS, TOPK, CAP, 1))(expert_ids_keys, expert_ids_turns).reshape((TOKENS, TOPK))
    route_weights = jnp.clip(0.2 + 0.8 * jax.random.uniform(key_list[23], (TOKENS, TOPK), jnp.float32) ** block_levels(key_list[23], (TOKENS, TOPK), ((0, 32),), -0.2, 0.2), 0.2, 1.0)
    return {"queries_narrow": queries_narrow, "keys_narrow": keys_narrow, "values_narrow": values_narrow, "queries_wide": queries_wide, "keys_wide": keys_wide, "values_wide": values_wide, "lambda_narrow": lambda_narrow, "lambda_wide": lambda_wide, "gain_narrow": gain_narrow, "gain_wide": gain_wide, "out_narrow": out_narrow, "out_wide": out_wide, "stream": stream, "gain_mix": gain_mix, "gain_ffn": gain_ffn, "gain_post": gain_post, "shared_gate": shared_gate, "shared_up": shared_up, "shared_down": shared_down, "expert_gate": expert_gate, "expert_up": expert_up, "expert_down": expert_down, "expert_ids": expert_ids, "route_weights": route_weights}


EPS = 1e-06

def rms_scale(values, gain_row):
    return values * lax.rsqrt(lax.optimization_barrier(jnp.mean(values * values, axis=-1, keepdims=True)) + EPS) * gain_row

def round_trip(values):
    return lax.optimization_barrier(values.astype(jnp.bfloat16)).astype(jnp.float32)

def group_attention(queries, keys, values, lam_heads, gain_row, heads, groups, key_dim, value_dim):
    per_group = heads // groups
    length = queries.shape[0]
    blocks = length // TOK_DEV
    query_blocks = queries.reshape(blocks, TOK_DEV, groups, per_group, 2, key_dim)
    key_rows = keys.reshape(length, groups, 2, key_dim).astype(jnp.float32)
    value_rows = values.reshape(length, groups, value_dim).astype(jnp.float32)
    key_pos = jnp.arange(length, dtype=jnp.int32)
    lam_grid = lam_heads.reshape(groups, per_group)[:, :, None, None]

    def one_block(inputs):
        query_block, block_index = inputs
        query_pos = block_index * TOK_DEV + jnp.arange(TOK_DEV, dtype=jnp.int32)
        scores = jnp.einsum('qcgmd,kcmd->cgmqk', query_block.astype(jnp.float32), key_rows) * key_dim ** (-0.5)
        causal = key_pos[None, :] <= query_pos[:, None]
        scores = jnp.where(causal, scores, -1e+30)
        row_max = lax.optimization_barrier(jnp.max(scores, axis=-1, keepdims=True))
        weights = jnp.where(causal, jnp.exp(scores - row_max), 0.0)
        row_sum = lax.optimization_barrier(jnp.sum(weights, axis=-1))
        summed_values = jnp.einsum('cgmqk,kcv->cgmqv', round_trip(weights), value_rows)
        mapped = summed_values / row_sum[..., None]
        difference = mapped[:, :, 0] - lam_grid * mapped[:, :, 1]
        normed = rms_scale(difference, gain_row)
        return normed.transpose(2, 0, 1, 3).reshape(TOK_DEV, heads * value_dim).astype(jnp.bfloat16)
    outputs = lax.map(one_block, (query_blocks, jnp.arange(blocks, dtype=jnp.int32)))
    return outputs.reshape(length, heads * value_dim)

def routed_sum(normed, expert_gate, expert_up, expert_down, expert_ids, route_weights):
    assignments = TOKENS * TOPK
    flat_ids = expert_ids.reshape(-1)
    flat_weights = jnp.concatenate([route_weights.reshape(-1), jnp.zeros((1,), jnp.float32)])
    padded = jnp.concatenate([normed, jnp.zeros((1, D), jnp.bfloat16)], axis=0)
    row_bound = N_SP * N_TP * CAP
    half_width = FF // N_TP

    def per_expert(carried, expert):
        matches = jnp.nonzero(flat_ids == expert, size=row_bound, fill_value=assignments)[0].astype(jnp.int32)
        tokens_hit = matches // TOPK
        rows_in = padded[tokens_hit]
        gate_all = lax.dynamic_index_in_dim(expert_gate, expert, 0, keepdims=False)
        up_all = lax.dynamic_index_in_dim(expert_up, expert, 0, keepdims=False)
        down_all = lax.dynamic_index_in_dim(expert_down, expert, 0, keepdims=False)
        summed = jnp.zeros((row_bound, D), jnp.float32)
        for part_index in range(N_TP):
            low = part_index * half_width
            gate_cols = gate_all[:, low:low + half_width]
            up_cols = up_all[:, low:low + half_width]
            down_rows = down_all[low:low + half_width]
            hidden = (jax.nn.silu(jnp.dot(rows_in, gate_cols, preferred_element_type=jnp.float32)) * jnp.dot(rows_in, up_cols, preferred_element_type=jnp.float32)).astype(jnp.bfloat16)
            summed = summed + round_trip(jnp.dot(hidden, down_rows, preferred_element_type=jnp.float32))
        expert_out = round_trip(summed)
        weighted = expert_out * flat_weights[matches][:, None]
        return (carried.at[tokens_hit].add(weighted, mode='drop'), None)
    routed, unused = lax.scan(per_expert, jnp.zeros((TOKENS, D), jnp.float32), jnp.arange(EXPERTS, dtype=jnp.int32))
    return routed

def reference(queries_narrow, keys_narrow, values_narrow, queries_wide, keys_wide, values_wide, lambda_narrow, lambda_wide, gain_narrow, gain_wide, out_narrow, out_wide, stream, gain_mix, gain_ffn, gain_post, shared_gate, shared_up, shared_down, expert_gate, expert_up, expert_down, expert_ids, route_weights):
    narrow = group_attention(queries_narrow, keys_narrow, values_narrow, lambda_narrow, gain_narrow, HN, KN, DN, VN)
    wide = group_attention(queries_wide, keys_wide, values_wide, lambda_wide, gain_wide, HW, KW, DW, VW)
    projected = jnp.dot(narrow, out_narrow, preferred_element_type=jnp.float32) + jnp.dot(wide, out_wide, preferred_element_type=jnp.float32)
    mixed_rows = (stream.astype(jnp.float32) + rms_scale(projected, gain_mix)).astype(jnp.bfloat16)
    normed = rms_scale(mixed_rows.astype(jnp.float32), gain_ffn).astype(jnp.bfloat16)
    shared_hidden = (jax.nn.silu(jnp.dot(normed, shared_gate, preferred_element_type=jnp.float32)) * jnp.dot(normed, shared_up, preferred_element_type=jnp.float32)).astype(jnp.bfloat16)
    shared_out = jnp.dot(shared_hidden, shared_down, preferred_element_type=jnp.float32)
    routed = routed_sum(normed, expert_gate, expert_up, expert_down, expert_ids, route_weights)
    combined = shared_out + routed
    return (mixed_rows.astype(jnp.float32) + rms_scale(combined, gain_post)).astype(jnp.bfloat16)
```

```python
import functools
import math

import jax
import jax.numpy as jnp
from jax import lax
from jax.experimental import pallas as pl
from jax.experimental.pallas import tpu as pltpu
from jax.sharding import PartitionSpec as P

D = 2048
DN = 64
VN = 128
DW = 128
VW = 256
TOPK = 4


EPS = 1e-06


def rms_scale(values, gain_row):
    return values * lax.rsqrt(jnp.mean(values * values, axis=-1, keepdims=True) + EPS) * gain_row


MESH = pl.DeviceIdType.MESH
LOG2E = math.log2(math.e)
MASKED = -1e30


def plane_shape(sp_count):
    bits = sp_count.bit_length() - 1
    if 1 << bits != sp_count:
        return sp_count, 1, 1
    columns = 1 << (bits // 3 if bits % 3 == 0 else (bits - bits // 2) // 2)
    rows = columns
    return sp_count // (rows * columns), rows, columns


def attend_kernel(
    dims,
    qn_ref,
    kn_ref,
    vn_ref,
    qw_ref,
    kw_ref,
    vw_ref,
    lamn_ref,
    lamw_ref,
    gainn_ref,
    gainw_ref,
    out_ref,
    kv,
    att,
    row_max,
    row_sum,
    acc_n,
    acc_w,
    load_sem,
    recv_sem,
    up_sem,
    first_sem,
    second_sem,
    pair_send,
    pair_recv,
    pair_ready,
):
    planes, rows, columns, tp_count = dims
    per_plane = rows * columns
    sp = lax.axis_index("sp")
    tp = lax.axis_index("tp")
    plane = sp // per_plane
    cell = sp % per_plane
    y = cell // columns
    x = cell % columns
    queries = qn_ref.shape[2]
    half_rows = queries // 2

    own = []
    begin = 0
    for index, ref in enumerate((kn_ref, vn_ref, kw_ref, vw_ref)):
        width = ref.shape[1]
        own.append(
            pltpu.make_async_copy(ref, kv.at[0, cell, :, pl.ds(begin, width)], load_sem.at[index])
        )
        begin += width
    for copy in own:
        copy.start()

    def line(axis):
        if axis == 0:
            return [((y + k) % rows) * columns + x for k in range(1, rows)]
        return [y * columns + (x + k) % columns for k in range(1, columns)]

    def crossed(other, axis):
        oy = other // columns
        ox = other % columns
        if axis == 0:
            return [((oy + k) % rows) * columns + ox for k in range(1, rows)]
        return [oy * columns + (ox + k) % columns for k in range(1, columns)]

    barrier = pltpu.get_barrier_semaphore()
    for other in line(0) + line(1):
        pl.semaphore_signal(
            barrier, inc=1, device_id={"sp": plane * per_plane + other}, device_id_type=MESH
        )
    for k in range(1, tp_count):
        pl.semaphore_signal(
            barrier, inc=1, device_id={"tp": (tp + k) % tp_count}, device_id_type=MESH
        )

    @pl.when(plane > 0)
    def _():
        pl.semaphore_signal(barrier, inc=1, device_id={"sp": sp - per_plane}, device_id_type=MESH)

    @pl.when(plane < planes - 1)
    def _():
        pl.semaphore_signal(barrier, inc=1, device_id={"sp": sp + per_plane}, device_id_type=MESH)

    below = (plane > 0).astype(jnp.int32)
    above = (plane < planes - 1).astype(jnp.int32)
    pl.semaphore_wait(barrier, rows - 1 + columns - 1 + tp_count - 1 + below + above)

    for copy in own:
        copy.wait()

    def piece(depth, block, half):
        return kv.at[depth, block, pl.ds(half * half_rows, half_rows), :]

    def remote(depth, to_depth, block, half, target, send):
        return pltpu.make_async_remote_copy(
            src_ref=piece(depth, block, half),
            dst_ref=piece(to_depth, block, half),
            send_sem=send,
            recv_sem=recv_sem.at[to_depth, block, half],
            device_id={"sp": target},
            device_id_type=MESH,
        )

    def arrived(depth, block, half):
        pltpu.make_async_remote_copy(
            src_ref=piece(depth, block, half),
            dst_ref=piece(depth, block, half),
            send_sem=up_sem.at[0, 0],
            recv_sem=recv_sem.at[depth, block, half],
            device_id={"sp": sp},
            device_id_type=MESH,
        ).wait_recv()

    def up_copies(depth):
        return [
            remote(depth, depth + 1, cell, half, sp + per_plane, up_sem.at[depth, half])
            for half in range(2)
        ]

    def direct_copies(depth):
        copies = []
        for half in range(2):
            for k, other in enumerate(line(half)):
                copies.append(
                    remote(
                        depth,
                        depth,
                        cell,
                        half,
                        plane * per_plane + other,
                        first_sem.at[depth, half, k],
                    )
                )
            for k, other in enumerate(line(1 - half)):
                copies.append(
                    remote(
                        depth,
                        depth,
                        cell,
                        half,
                        plane * per_plane + other,
                        second_sem.at[depth, half, 0, k],
                    )
                )
        return copies

    def relay_copies(depth):
        groups = []
        for half in range(2):
            for i, block in enumerate(line(half)):
                copies = [
                    remote(
                        depth,
                        depth,
                        block,
                        half,
                        plane * per_plane + other,
                        second_sem.at[depth, half, i + 1, k],
                    )
                    for k, other in enumerate(line(1 - half))
                ]
                groups.append((block, half, copies))
        return groups

    def issue(depth):
        @pl.when(plane < planes - 1)
        def _():
            for copy in up_copies(depth):
                copy.start()

        for copy in direct_copies(depth):
            copy.start()

    def relay(depth):
        for block, half, copies in relay_copies(depth):
            arrived(depth, block, half)
            for copy in copies:
                copy.start()

    def finish(depth):
        for half in range(2):
            for block in line(1 - half):
                arrived(depth, block, half)
            for first in line(half):
                for block in crossed(first, 1 - half):
                    arrived(depth, block, half)

    row_max[...] = jnp.full_like(row_max, MASKED)
    row_sum[...] = jnp.zeros_like(row_sum)
    acc_n[...] = jnp.zeros_like(acc_n)
    acc_w[...] = jnp.zeros_like(acc_w)
    heads_n = qn_ref.shape[0]
    heads_w = qw_ref.shape[1] // kw_ref.shape[1]
    width_k = kn_ref.shape[1]
    value_n = vn_ref.shape[1]
    begin_kw = width_k + value_n
    map_w = kw_ref.shape[1] // 2
    begin_vw = begin_kw + 2 * map_w
    value_w = vw_ref.shape[1]
    chunk = math.gcd(per_plane, 4)
    key_rows = chunk * queries

    def tile(query, key, value, factor, mask, state, acc, slot):
        scores = lax.dot_general(
            query, key, (((1,), (1,)), ((), ())), preferred_element_type=jnp.float32
        )
        if mask is not None:
            scores = jnp.where(mask, scores, MASKED)
        before = row_max[state][:, :1]
        now = jnp.maximum(before, jnp.max(scores, axis=1, keepdims=True))
        weights = jnp.exp2((scores - now) * factor)
        decay = jnp.exp2((before - now) * factor)
        total = row_sum[state][:, :1] * decay + jnp.sum(weights, axis=1, keepdims=True)
        acc[slot] = acc[slot] * decay + jnp.dot(
            weights.astype(jnp.bfloat16), value, preferred_element_type=jnp.float32
        )
        row_max[state] = jnp.broadcast_to(now, row_max.shape[1:])
        row_sum[state] = jnp.broadcast_to(total, row_sum.shape[1:])

    def attend(depth, masked):
        def part(at):
            def columns_of(begin, width):
                return kv[depth, pl.ds(at, chunk), :, begin : begin + width].reshape(
                    key_rows, width
                )

            mask = None
            if masked:
                query_pos = cell * queries + lax.broadcasted_iota(
                    jnp.int32, (queries, key_rows), 0
                )
                key_pos = at * queries + lax.broadcasted_iota(jnp.int32, (queries, key_rows), 1)
                mask = key_pos <= query_pos

            def narrow(head, carry):
                key = columns_of(0, width_k)
                value = columns_of(width_k, value_n)
                for which in range(2):
                    index = head * 2 + which
                    tile(
                        qn_ref[head, which],
                        key,
                        value,
                        DN**-0.5 * LOG2E,
                        mask,
                        index,
                        acc_n,
                        index,
                    )
                return carry

            def wide(head, carry):
                value = columns_of(begin_vw, value_w)
                for which in range(2):
                    index = head * 2 + which
                    tile(
                        qw_ref[:, pl.ds(pl.multiple_of(index * map_w, map_w), map_w)],
                        columns_of(begin_kw + which * map_w, map_w),
                        value,
                        DW**-0.5 * LOG2E,
                        mask,
                        2 * heads_n + index,
                        acc_w,
                        index,
                    )
                return carry

            lax.fori_loop(0, heads_n, narrow, 0)
            lax.fori_loop(0, heads_w, wide, 0)

        if per_plane == chunk:
            part(0)
        else:

            def step(at, carry):
                part(at * chunk)
                return carry

            lax.fori_loop(0, per_plane // chunk, step, 0)

    def advance(depth):
        @pl.when(depth < plane)
        def _():
            for half in range(2):
                arrived(depth + 1, cell, half)
            issue(depth + 1)

    def relay_next(depth):
        @pl.when(depth < plane)
        def _():
            relay(depth + 1)

    issue(0)
    relay(0)
    advance(0)
    finish(0)
    attend(0, True)
    relay_next(0)

    def depth_step(depth, carry):
        advance(depth)
        finish(depth)
        attend(depth, False)
        relay_next(depth)
        return carry

    lax.fori_loop(1, plane + 1, depth_step, 0)

    def close(first, second, lam, gain):
        head = first - lam * second
        scale = lax.rsqrt(jnp.mean(head * head, axis=1, keepdims=True) + EPS)
        return (head * scale * gain).astype(jnp.bfloat16)

    for head in range(heads_n):
        maps = [acc_n[2 * head + k] / row_sum[2 * head + k][:, :1] for k in range(2)]
        att[:, head * value_n : (head + 1) * value_n] = close(
            maps[0], maps[1], lamn_ref[head], gainn_ref[...]
        )
    begin_w = heads_n * value_n
    for head in range(heads_w):
        maps = [
            acc_w[2 * head + k] / row_sum[2 * (heads_n + head) + k][:, :1] for k in range(2)
        ]
        att[:, begin_w + head * value_w : begin_w + (head + 1) * value_w] = close(
            maps[0], maps[1], lamw_ref[head], gainw_ref[...]
        )

    def drain(depth, carry):
        @pl.when(plane < planes - 1)
        def _():
            for copy in up_copies(depth):
                copy.wait_send()

        for copy in direct_copies(depth):
            copy.wait_send()
        for _block, _half, copies in relay_copies(depth):
            for copy in copies:
                copy.wait_send()
        return carry

    lax.fori_loop(0, plane + 1, drain, 0)
    for k in range(1, tp_count):
        pl.semaphore_signal(
            pair_ready, inc=1, device_id={"tp": (tp + k) % tp_count}, device_id_type=MESH
        )
    pl.semaphore_wait(pair_ready, tp_count - 1)
    share = out_ref.shape[1]
    copies = []
    for k in range(1, tp_count):
        other = (tp + k) % tp_count
        copies.append(
            pltpu.make_async_remote_copy(
                src_ref=att.at[pl.ds(pl.multiple_of(other * share, share), share), :],
                dst_ref=out_ref.at[tp],
                send_sem=pair_send.at[k - 1],
                recv_sem=pair_recv.at[k - 1],
                device_id={"tp": other},
                device_id_type=MESH,
            )
        )
    for copy in copies:
        copy.start()
    out_ref[tp] = att[pl.ds(pl.multiple_of(tp * share, share), share), :]
    for copy in copies:
        copy.wait()


def attended_rows(
    sp_count,
    tp_count,
    queries_narrow,
    keys_narrow,
    values_narrow,
    queries_wide,
    keys_wide,
    values_wide,
    lambda_narrow,
    lambda_wide,
    gain_narrow,
    gain_wide,
):
    planes, rows, columns = plane_shape(sp_count)
    count = queries_narrow.shape[0]
    heads_n = queries_narrow.shape[1] // (2 * DN)
    heads_w = queries_wide.shape[1] // (2 * DW)
    maps = queries_narrow.reshape(count, heads_n, 2, DN).transpose(1, 2, 0, 3)
    padded = jnp.stack(
        [
            jnp.pad(maps[:, 0], ((0, 0), (0, 0), (0, DN))),
            jnp.pad(maps[:, 1], ((0, 0), (0, 0), (DN, 0))),
        ],
        axis=1,
    )
    width = (
        keys_narrow.shape[1] + values_narrow.shape[1] + keys_wide.shape[1] + values_wide.shape[1]
    )
    per_plane = rows * columns
    features = heads_n * VN + heads_w * VW
    longest = max(rows, columns)
    tiles = 2 * (heads_n + heads_w)
    vmem = pl.BlockSpec(memory_space=pltpu.VMEM)
    smem = pl.BlockSpec(memory_space=pltpu.SMEM)
    hbm = pl.BlockSpec(memory_space=pl.ANY)
    return pl.pallas_call(
        functools.partial(attend_kernel, (planes, rows, columns, tp_count)),
        out_shape=jax.ShapeDtypeStruct((tp_count, count // tp_count, features), jnp.bfloat16),
        in_specs=[vmem, hbm, hbm, vmem, hbm, hbm, smem, smem, vmem, vmem],
        out_specs=vmem,
        scratch_shapes=[
            pltpu.VMEM((planes, per_plane, count, width), jnp.bfloat16),
            pltpu.VMEM((count, features), jnp.bfloat16),
            pltpu.VMEM((tiles, count, 128), jnp.float32),
            pltpu.VMEM((tiles, count, 128), jnp.float32),
            pltpu.VMEM((2 * heads_n, count, VN), jnp.float32),
            pltpu.VMEM((2 * heads_w, count, VW), jnp.float32),
            pltpu.SemaphoreType.DMA((4,)),
            pltpu.SemaphoreType.DMA((planes, per_plane, 2)),
            pltpu.SemaphoreType.DMA((planes, 2)),
            pltpu.SemaphoreType.DMA((planes, 2, longest)),
            pltpu.SemaphoreType.DMA((planes, 2, longest, longest)),
            pltpu.SemaphoreType.DMA((max(1, tp_count - 1),)),
            pltpu.SemaphoreType.DMA((max(1, tp_count - 1),)),
            pltpu.SemaphoreType.REGULAR,
        ],
        compiler_params=pltpu.CompilerParams(
            collective_id=0, has_side_effects=True, vmem_limit_bytes=56 * 1024 * 1024
        ),
        name="gather_attend",
    )(
        padded,
        keys_narrow,
        values_narrow,
        queries_wide,
        keys_wide,
        values_wide,
        lambda_narrow,
        lambda_wide,
        gain_narrow.reshape(1, -1),
        gain_wide.reshape(1, -1),
    )


def run_experts(incoming, expert_gate, expert_up, expert_down, capacity):
    sources = incoming.shape[0]
    local_experts = expert_gate.shape[0]
    grouped = incoming.reshape(sources, local_experts, capacity, D)
    gate_part = jnp.einsum(
        "rjcd,jdf->rjcf", grouped, expert_gate, preferred_element_type=jnp.float32
    )
    up_part = jnp.einsum("rjcd,jdf->rjcf", grouped, expert_up, preferred_element_type=jnp.float32)
    hidden = (jax.nn.silu(gate_part) * up_part).astype(jnp.bfloat16)
    result = jnp.einsum("rjcf,jfd->rjcd", hidden, expert_down, preferred_element_type=jnp.float32)
    return result.reshape(sources, local_experts * capacity, D)


def shards(
    queries_narrow,
    keys_narrow,
    values_narrow,
    queries_wide,
    keys_wide,
    values_wide,
    lambda_narrow,
    lambda_wide,
    gain_narrow,
    gain_wide,
    out_narrow,
    out_wide,
    stream,
    gain_mix,
    gain_ffn,
    gain_post,
    shared_gate,
    shared_up,
    shared_down,
    expert_gate,
    expert_up,
    expert_down,
    expert_ids,
    route_weights,
):
    sp_count = lax.axis_size("sp")
    attended = attended_rows(
        sp_count,
        lax.axis_size("tp"),
        queries_narrow,
        keys_narrow,
        values_narrow,
        queries_wide,
        keys_wide,
        values_wide,
        lambda_narrow,
        lambda_wide,
        gain_narrow,
        gain_wide,
    )
    narrow_width = out_narrow.shape[0] // attended.shape[0]
    attended = attended.transpose(1, 0, 2)
    narrow_rows = attended[:, :, :narrow_width].reshape(attended.shape[0], -1)
    wide_rows = attended[:, :, narrow_width:].reshape(attended.shape[0], -1)
    projected = jnp.dot(narrow_rows, out_narrow, preferred_element_type=jnp.float32) + jnp.dot(
        wide_rows, out_wide, preferred_element_type=jnp.float32
    )
    mixed_rows = (stream.astype(jnp.float32) + rms_scale(projected, gain_mix)).astype(jnp.bfloat16)
    normed = rms_scale(mixed_rows.astype(jnp.float32), gain_ffn).astype(jnp.bfloat16)
    row_count = normed.shape[0]
    tp_count = lax.axis_size("tp")
    local_experts = expert_gate.shape[0]
    experts_all = local_experts * sp_count
    capacity = max(2, 3 * row_count * TOPK // (2 * experts_all))
    flat_ids = expert_ids.reshape(-1)
    onehot = (flat_ids[:, None] == jnp.arange(experts_all, dtype=jnp.int32)[None, :]).astype(
        jnp.int32
    )
    earlier = jnp.cumsum(onehot, axis=0) - onehot
    slot_rank = jnp.sum(earlier * onehot, axis=1)
    slot_index = flat_ids * capacity + slot_rank
    buffer_rows = experts_all * capacity
    selector = slot_index[None, :] == jnp.arange(buffer_rows, dtype=jnp.int32)[:, None]
    selector = jnp.any(selector.reshape(buffer_rows, row_count, TOPK), axis=2).astype(jnp.bfloat16)
    outgoing = jnp.dot(selector, normed, preferred_element_type=jnp.float32).astype(jnp.bfloat16)
    outgoing = outgoing.reshape(sp_count, local_experts * capacity, D)
    incoming = lax.all_to_all(outgoing, "sp", split_axis=0, concat_axis=0, tiled=True)
    all_rows = lax.all_gather(incoming[None], "tp", axis=0, tiled=True)
    partials = run_experts(
        all_rows.reshape(tp_count * sp_count, local_experts * capacity, D),
        expert_gate,
        expert_up,
        expert_down,
        capacity,
    )
    partials = partials.reshape(tp_count, sp_count, local_experts * capacity, D)
    own_sums = lax.psum_scatter(
        partials.astype(jnp.bfloat16), "tp", scatter_dimension=0, tiled=True
    ).astype(jnp.float32)
    returned = lax.all_to_all(
        own_sums[0].astype(jnp.bfloat16), "sp", split_axis=0, concat_axis=0, tiled=True
    )
    returned = returned.reshape(buffer_rows, D)
    picked = jnp.take(returned, slot_index, axis=0).reshape(row_count, TOPK, D)
    routed = jnp.einsum(
        "rk,rkd->rd", route_weights, picked.astype(jnp.float32), precision=lax.Precision.HIGHEST
    )
    shared_hidden = (
        jax.nn.silu(jnp.dot(normed, shared_gate, preferred_element_type=jnp.float32))
        * jnp.dot(normed, shared_up, preferred_element_type=jnp.float32)
    ).astype(jnp.bfloat16)
    shared_out = jnp.dot(shared_hidden, shared_down, preferred_element_type=jnp.float32)
    combined = shared_out + routed
    return (mixed_rows.astype(jnp.float32) + rms_scale(combined, gain_post)).astype(jnp.bfloat16)


def solution(mesh):
    return jax.shard_map(
        shards,
        mesh=mesh,
        in_specs=(
            P("sp", "tp"),
            P("sp", "tp"),
            P("sp", "tp"),
            P("sp", "tp"),
            P("sp", "tp"),
            P("sp", "tp"),
            P("tp"),
            P("tp"),
            P(),
            P(),
            P(),
            P(),
            P(("sp", "tp"), None),
            P(),
            P(),
            P(),
            P(),
            P(),
            P(),
            P("sp", None, "tp"),
            P("sp", None, "tp"),
            P("sp", "tp", None),
            P(("sp", "tp"), None),
            P(("sp", "tp"), None),
        ),
        out_specs=P(("sp", "tp"), None),
        check_vma=False,
    )
```

```python
import functools
import math

import jax
import jax.numpy as jnp
from jax import lax
from jax.experimental import pallas as pl
from jax.experimental.pallas import tpu as pltpu
from jax.sharding import PartitionSpec as P

D = 2048
DN = 64
VN = 128
DW = 128
VW = 256
TOPK = 4


EPS = 1e-06


def rms_scale(values, gain_row):
    return values * lax.rsqrt(jnp.mean(values * values, axis=-1, keepdims=True) + EPS) * gain_row


MESH = pl.DeviceIdType.MESH
LOG2E = math.log2(math.e)
MASKED = -1e30


def plane_shape(sp_count):
    bits = sp_count.bit_length() - 1
    if 1 << bits != sp_count:
        return sp_count, 1, 1
    columns = 1 << (bits // 3 if bits % 3 == 0 else (bits - bits // 2) // 2)
    rows = columns
    return sp_count // (rows * columns), rows, columns


def attend_kernel(
    dims,
    qn_ref,
    kn_ref,
    vn_ref,
    qw_ref,
    kw_ref,
    vw_ref,
    lamn_ref,
    lamw_ref,
    gainn_ref,
    gainw_ref,
    out_ref,
    kv,
    att,
    row_max,
    row_sum,
    acc_n,
    acc_w,
    load_sem,
    recv_sem,
    up_sem,
    first_sem,
    second_sem,
    pair_send,
    pair_recv,
    pair_ready,
):
    planes, rows, columns, tp_count = dims
    per_plane = rows * columns
    sp = lax.axis_index("sp")
    tp = lax.axis_index("tp")
    plane = sp // per_plane
    cell = sp % per_plane
    y = cell // columns
    x = cell % columns
    queries = qn_ref.shape[2]
    half_rows = queries // 2

    own = []
    begin = 0
    for index, ref in enumerate((kn_ref, vn_ref, kw_ref, vw_ref)):
        width = ref.shape[1]
        own.append(
            pltpu.make_async_copy(ref, kv.at[0, cell, :, pl.ds(begin, width)], load_sem.at[index])
        )
        begin += width
    for copy in own:
        copy.start()

    def line(axis):
        if axis == 0:
            return [((y + k) % rows) * columns + x for k in range(1, rows)]
        return [y * columns + (x + k) % columns for k in range(1, columns)]

    def crossed(other, axis):
        oy = other // columns
        ox = other % columns
        if axis == 0:
            return [((oy + k) % rows) * columns + ox for k in range(1, rows)]
        return [oy * columns + (ox + k) % columns for k in range(1, columns)]

    barrier = pltpu.get_barrier_semaphore()
    for other in line(0) + line(1):
        pl.semaphore_signal(
            barrier, inc=1, device_id={"sp": plane * per_plane + other}, device_id_type=MESH
        )
    for k in range(1, tp_count):
        pl.semaphore_signal(
            barrier, inc=1, device_id={"tp": (tp + k) % tp_count}, device_id_type=MESH
        )

    @pl.when(plane > 0)
    def _():
        pl.semaphore_signal(barrier, inc=1, device_id={"sp": sp - per_plane}, device_id_type=MESH)

    @pl.when(plane < planes - 1)
    def _():
        pl.semaphore_signal(barrier, inc=1, device_id={"sp": sp + per_plane}, device_id_type=MESH)

    below = (plane > 0).astype(jnp.int32)
    above = (plane < planes - 1).astype(jnp.int32)
    pl.semaphore_wait(barrier, rows - 1 + columns - 1 + tp_count - 1 + below + above)

    for copy in own:
        copy.wait()

    def piece(depth, block, half):
        return kv.at[depth, block, pl.ds(half * half_rows, half_rows), :]

    def remote(depth, to_depth, block, half, target, send):
        return pltpu.make_async_remote_copy(
            src_ref=piece(depth, block, half),
            dst_ref=piece(to_depth, block, half),
            send_sem=send,
            recv_sem=recv_sem.at[to_depth, block, half],
            device_id={"sp": target},
            device_id_type=MESH,
        )

    def arrived(depth, block, half):
        pltpu.make_async_remote_copy(
            src_ref=piece(depth, block, half),
            dst_ref=piece(depth, block, half),
            send_sem=up_sem.at[0, 0],
            recv_sem=recv_sem.at[depth, block, half],
            device_id={"sp": sp},
            device_id_type=MESH,
        ).wait_recv()

    def up_copies(depth):
        return [
            remote(depth, depth + 1, cell, half, sp + per_plane, up_sem.at[depth, half])
            for half in range(2)
        ]

    def direct_copies(depth):
        copies = []
        for half in range(2):
            for k, other in enumerate(line(half)):
                copies.append(
                    remote(
                        depth,
                        depth,
                        cell,
                        half,
                        plane * per_plane + other,
                        first_sem.at[depth, half, k],
                    )
                )
            for k, other in enumerate(line(1 - half)):
                copies.append(
                    remote(
                        depth,
                        depth,
                        cell,
                        half,
                        plane * per_plane + other,
                        second_sem.at[depth, half, 0, k],
                    )
                )
        return copies

    def relay_copies(depth):
        groups = []
        for half in range(2):
            for i, block in enumerate(line(half)):
                copies = [
                    remote(
                        depth,
                        depth,
                        block,
                        half,
                        plane * per_plane + other,
                        second_sem.at[depth, half, i + 1, k],
                    )
                    for k, other in enumerate(line(1 - half))
                ]
                groups.append((block, half, copies))
        return groups

    def issue(depth):
        @pl.when(plane < planes - 1)
        def _():
            for copy in up_copies(depth):
                copy.start()

        for copy in direct_copies(depth):
            copy.start()

    def relay(depth):
        for block, half, copies in relay_copies(depth):
            arrived(depth, block, half)
            for copy in copies:
                copy.start()

    def finish(depth):
        for half in range(2):
            for block in line(1 - half):
                arrived(depth, block, half)
            for first in line(half):
                for block in crossed(first, 1 - half):
                    arrived(depth, block, half)

    row_max[...] = jnp.full_like(row_max, MASKED)
    row_sum[...] = jnp.zeros_like(row_sum)
    acc_n[...] = jnp.zeros_like(acc_n)
    acc_w[...] = jnp.zeros_like(acc_w)
    heads_n = qn_ref.shape[0]
    heads_w = qw_ref.shape[1] // kw_ref.shape[1]
    width_k = kn_ref.shape[1]
    value_n = vn_ref.shape[1]
    begin_kw = width_k + value_n
    map_w = kw_ref.shape[1] // 2
    begin_vw = begin_kw + 2 * map_w
    value_w = vw_ref.shape[1]
    chunk = math.gcd(per_plane, 4)
    key_rows = chunk * queries

    def tile(query, key, value, factor, mask, state, acc, slot):
        scores = lax.dot_general(
            query, key, (((1,), (1,)), ((), ())), preferred_element_type=jnp.float32
        )
        if mask is not None:
            scores = jnp.where(mask, scores, MASKED)
        before = row_max[state][:, :1]
        now = jnp.maximum(before, jnp.max(scores, axis=1, keepdims=True))
        weights = jnp.exp2((scores - now) * factor)
        decay = jnp.exp2((before - now) * factor)
        total = row_sum[state][:, :1] * decay + jnp.sum(weights, axis=1, keepdims=True)
        acc[slot] = acc[slot] * decay + jnp.dot(
            weights.astype(jnp.bfloat16), value, preferred_element_type=jnp.float32
        )
        row_max[state] = jnp.broadcast_to(now, row_max.shape[1:])
        row_sum[state] = jnp.broadcast_to(total, row_sum.shape[1:])

    def attend(depth, masked):
        def part(at):
            def columns_of(begin, width):
                return kv[depth, pl.ds(at, chunk), :, begin : begin + width].reshape(
                    key_rows, width
                )

            mask = None
            if masked:
                query_pos = cell * queries + lax.broadcasted_iota(
                    jnp.int32, (queries, key_rows), 0
                )
                key_pos = at * queries + lax.broadcasted_iota(jnp.int32, (queries, key_rows), 1)
                mask = key_pos <= query_pos

            def narrow(head, carry):
                key = columns_of(0, width_k)
                value = columns_of(width_k, value_n)
                for which in range(2):
                    index = head * 2 + which
                    tile(
                        qn_ref[head, which],
                        key,
                        value,
                        DN**-0.5 * LOG2E,
                        mask,
                        index,
                        acc_n,
                        index,
                    )
                return carry

            def wide(head, carry):
                value = columns_of(begin_vw, value_w)
                for which in range(2):
                    index = head * 2 + which
                    tile(
                        qw_ref[:, pl.ds(pl.multiple_of(index * map_w, map_w), map_w)],
                        columns_of(begin_kw + which * map_w, map_w),
                        value,
                        DW**-0.5 * LOG2E,
                        mask,
                        2 * heads_n + index,
                        acc_w,
                        index,
                    )
                return carry

            lax.fori_loop(0, heads_n, narrow, 0)
            lax.fori_loop(0, heads_w, wide, 0)

        if per_plane == chunk:
            part(0)
        else:

            def step(at, carry):
                part(at * chunk)
                return carry

            lax.fori_loop(0, per_plane // chunk, step, 0)

    def advance(depth):
        @pl.when(depth < plane)
        def _():
            for half in range(2):
                arrived(depth + 1, cell, half)
            issue(depth + 1)

    def relay_next(depth):
        @pl.when(depth < plane)
        def _():
            relay(depth + 1)

    issue(0)
    relay(0)
    advance(0)
    finish(0)
    attend(0, True)
    relay_next(0)

    def depth_step(depth, carry):
        advance(depth)
        finish(depth)
        attend(depth, False)
        relay_next(depth)
        return carry

    lax.fori_loop(1, plane + 1, depth_step, 0)

    def close(first, second, lam, gain):
        head = first - lam * second
        scale = lax.rsqrt(jnp.mean(head * head, axis=1, keepdims=True) + EPS)
        return (head * scale * gain).astype(jnp.bfloat16)

    for head in range(heads_n):
        maps = [acc_n[2 * head + k] / row_sum[2 * head + k][:, :1] for k in range(2)]
        att[:, head * value_n : (head + 1) * value_n] = close(
            maps[0], maps[1], lamn_ref[head], gainn_ref[...]
        )
    begin_w = heads_n * value_n
    for head in range(heads_w):
        maps = [
            acc_w[2 * head + k] / row_sum[2 * (heads_n + head) + k][:, :1] for k in range(2)
        ]
        att[:, begin_w + head * value_w : begin_w + (head + 1) * value_w] = close(
            maps[0], maps[1], lamw_ref[head], gainw_ref[...]
        )

    def drain(depth, carry):
        @pl.when(plane < planes - 1)
        def _():
            for copy in up_copies(depth):
                copy.wait_send()

        for copy in direct_copies(depth):
            copy.wait_send()
        for _block, _half, copies in relay_copies(depth):
            for copy in copies:
                copy.wait_send()
        return carry

    lax.fori_loop(0, plane + 1, drain, 0)
    for k in range(1, tp_count):
        pl.semaphore_signal(
            pair_ready, inc=1, device_id={"tp": (tp + k) % tp_count}, device_id_type=MESH
        )
    pl.semaphore_wait(pair_ready, tp_count - 1)
    share = out_ref.shape[1]
    copies = []
    for k in range(1, tp_count):
        other = (tp + k) % tp_count
        copies.append(
            pltpu.make_async_remote_copy(
                src_ref=att.at[pl.ds(pl.multiple_of(other * share, share), share), :],
                dst_ref=out_ref.at[tp],
                send_sem=pair_send.at[k - 1],
                recv_sem=pair_recv.at[k - 1],
                device_id={"tp": other},
                device_id_type=MESH,
            )
        )
    for copy in copies:
        copy.start()
    out_ref[tp] = att[pl.ds(pl.multiple_of(tp * share, share), share), :]
    for copy in copies:
        copy.wait()


def attended_rows(
    sp_count,
    tp_count,
    queries_narrow,
    keys_narrow,
    values_narrow,
    queries_wide,
    keys_wide,
    values_wide,
    lambda_narrow,
    lambda_wide,
    gain_narrow,
    gain_wide,
):
    planes, rows, columns = plane_shape(sp_count)
    count = queries_narrow.shape[0]
    heads_n = queries_narrow.shape[1] // (2 * DN)
    heads_w = queries_wide.shape[1] // (2 * DW)
    maps = queries_narrow.reshape(count, heads_n, 2, DN).transpose(1, 2, 0, 3)
    padded = jnp.stack(
        [
            jnp.pad(maps[:, 0], ((0, 0), (0, 0), (0, DN))),
            jnp.pad(maps[:, 1], ((0, 0), (0, 0), (DN, 0))),
        ],
        axis=1,
    )
    width = (
        keys_narrow.shape[1] + values_narrow.shape[1] + keys_wide.shape[1] + values_wide.shape[1]
    )
    per_plane = rows * columns
    features = heads_n * VN + heads_w * VW
    longest = max(rows, columns)
    tiles = 2 * (heads_n + heads_w)
    vmem = pl.BlockSpec(memory_space=pltpu.VMEM)
    smem = pl.BlockSpec(memory_space=pltpu.SMEM)
    hbm = pl.BlockSpec(memory_space=pl.ANY)
    return pl.pallas_call(
        functools.partial(attend_kernel, (planes, rows, columns, tp_count)),
        out_shape=jax.ShapeDtypeStruct((tp_count, count // tp_count, features), jnp.bfloat16),
        in_specs=[vmem, hbm, hbm, vmem, hbm, hbm, smem, smem, vmem, vmem],
        out_specs=vmem,
        scratch_shapes=[
            pltpu.VMEM((planes, per_plane, count, width), jnp.bfloat16),
            pltpu.VMEM((count, features), jnp.bfloat16),
            pltpu.VMEM((tiles, count, 128), jnp.float32),
            pltpu.VMEM((tiles, count, 128), jnp.float32),
            pltpu.VMEM((2 * heads_n, count, VN), jnp.float32),
            pltpu.VMEM((2 * heads_w, count, VW), jnp.float32),
            pltpu.SemaphoreType.DMA((4,)),
            pltpu.SemaphoreType.DMA((planes, per_plane, 2)),
            pltpu.SemaphoreType.DMA((planes, 2)),
            pltpu.SemaphoreType.DMA((planes, 2, longest)),
            pltpu.SemaphoreType.DMA((planes, 2, longest, longest)),
            pltpu.SemaphoreType.DMA((max(1, tp_count - 1),)),
            pltpu.SemaphoreType.DMA((max(1, tp_count - 1),)),
            pltpu.SemaphoreType.REGULAR,
        ],
        compiler_params=pltpu.CompilerParams(
            collective_id=0, has_side_effects=True, vmem_limit_bytes=56 * 1024 * 1024
        ),
        name="gather_attend",
    )(
        padded,
        keys_narrow,
        values_narrow,
        queries_wide,
        keys_wide,
        values_wide,
        lambda_narrow,
        lambda_wide,
        gain_narrow.reshape(1, -1),
        gain_wide.reshape(1, -1),
    )


def plane_greeting(planes, rows, columns, tp_count):
    per_plane = rows * columns
    sp = lax.axis_index("sp")
    tp = lax.axis_index("tp")
    plane = sp // per_plane
    cell = sp % per_plane
    barrier = pltpu.get_barrier_semaphore()
    for k in range(1, per_plane):
        pl.semaphore_signal(
            barrier,
            inc=1,
            device_id={"sp": plane * per_plane + (cell + k) % per_plane},
            device_id_type=MESH,
        )
    for k in range(1, planes):
        pl.semaphore_signal(
            barrier,
            inc=1,
            device_id={"sp": (plane + k) % planes * per_plane + cell},
            device_id_type=MESH,
        )
    for k in range(1, tp_count):
        pl.semaphore_signal(
            barrier, inc=1, device_id={"tp": (tp + k) % tp_count}, device_id_type=MESH
        )
    pl.semaphore_wait(barrier, per_plane - 1 + planes - 1 + tp_count - 1)
    return plane, cell, sp, tp


def dispatch_kernel(
    dims,
    group,
    normed_ref,
    slots_ref,
    inbox,
    marks,
    held,
    stage,
    load_sem,
    row_recv,
    mark_recv,
    row_send,
    mark_send,
    cell_recv,
    cell_send,
    pair_recv,
    pair_send,
):
    planes, rows, columns, tp_count = dims
    per_plane = rows * columns
    sp_now = lax.axis_index("sp")
    mine = sp_now // per_plane
    loads = [
        pltpu.make_async_copy(normed_ref, held.at[mine], load_sem.at[0]),
        pltpu.make_async_copy(slots_ref, marks.at[mine], load_sem.at[1]),
    ]
    for copy in loads:
        copy.start()
    plane, cell, sp, tp = plane_greeting(planes, rows, columns, tp_count)
    for copy in loads:
        copy.wait()
    padded = stage.shape[2]
    token_count = held.shape[1]

    def hops(source, way):
        target = {"sp": (sp + per_plane * (1 if way == 0 else planes - 1)) % (planes * per_plane)}
        return [
            pltpu.make_async_remote_copy(
                src_ref=marks.at[source],
                dst_ref=marks.at[source],
                send_sem=mark_send.at[source, way],
                recv_sem=mark_recv.at[source],
                device_id=target,
                device_id_type=MESH,
            ),
            pltpu.make_async_remote_copy(
                src_ref=held.at[source],
                dst_ref=held.at[source],
                send_sem=row_send.at[source, way],
                recv_sem=row_recv.at[source],
                device_id=target,
                device_id_type=MESH,
            ),
        ]

    def to_cell(source, k):
        other = (cell + k) % per_plane
        return pltpu.make_async_remote_copy(
            src_ref=stage.at[source, other],
            dst_ref=inbox.at[tp, source * per_plane + cell],
            send_sem=cell_send.at[source, k],
            recv_sem=cell_recv.at[source, (per_plane - k) % per_plane],
            device_id={"sp": plane * per_plane + other},
            device_id_type=MESH,
        )

    def to_pair(source, k):
        block = inbox.at[tp, pl.ds(source * per_plane, per_plane)]
        return pltpu.make_async_remote_copy(
            src_ref=block,
            dst_ref=block,
            send_sem=pair_send.at[source, k - 1],
            recv_sem=pair_recv.at[source, k - 1],
            device_id={"tp": (tp + k) % tp_count},
            device_id_type=MESH,
        )

    steps = [(0, 0)] + [(d, way) for d in range(1, planes) for way in range(2)]

    def of_step(d, way):
        source = plane - d if way == 0 else plane + d
        exists = source >= 0 if way == 0 else source < planes
        return source, exists

    def onward(source, d, way, act):
        for side in ((0, 1) if d == 0 else (way,)):

            @pl.when(plane < planes - 1 if side == 0 else plane > 0)
            def _(side=side):
                for copy in hops(source, side):
                    act(copy)

    def start(copy):
        copy.start()

    def wait_send(copy):
        copy.wait_send()

    def body(d, way):
        source, exists = of_step(d, way)

        @pl.when(exists)
        def _():
            if d > 0:
                for copy in hops(source, way):
                    copy.wait_recv()
            onward(source, d, way, start)
            tokens = held[source]
            slots = marks[source]
            row = lax.broadcasted_iota(jnp.int32, (padded, token_count), 0)
            for k in list(range(1, per_plane)) + [0]:
                other = (cell + k) % per_plane
                base = (plane * per_plane + other) * group
                wanted = jnp.where(row < group, row + base, -1).astype(jnp.float32)
                hit = slots[0:1, :] == wanted
                for choice in range(1, TOPK):
                    hit = hit | (slots[choice : choice + 1, :] == wanted)
                chosen = jnp.dot(
                    jnp.where(hit, 1.0, 0.0).astype(jnp.bfloat16),
                    tokens,
                    preferred_element_type=jnp.float32,
                ).astype(jnp.bfloat16)
                if k == 0:
                    inbox[tp, source * per_plane + cell] = chosen
                else:
                    stage[source, other] = chosen
            for k in range(1, per_plane):
                to_cell(source, k).start()

    def finish(d, way):
        source, exists = of_step(d, way)

        @pl.when(exists)
        def _():
            for k in range(1, per_plane):
                pltpu.make_async_remote_copy(
                    src_ref=stage.at[source, cell],
                    dst_ref=inbox.at[tp, source * per_plane + (cell + k) % per_plane],
                    send_sem=cell_send.at[source, k],
                    recv_sem=cell_recv.at[source, k],
                    device_id={"sp": sp},
                    device_id_type=MESH,
                ).wait_recv()
            for k in range(1, tp_count):
                to_pair(source, k).start()

    for index, step in enumerate(steps):
        body(*step)
        if index > 0:
            finish(*steps[index - 1])
    finish(*steps[-1])
    for d, way in steps:
        source, exists = of_step(d, way)

        @pl.when(exists)
        def _(source=source, d=d, way=way):
            onward(source, d, way, wait_send)
            for k in range(1, per_plane):
                to_cell(source, k).wait_send()
            for k in range(1, tp_count):
                to_pair(source, k).wait()


def dispatched_rows(dims, group, normed, slot_index, route_weights):
    planes, rows, columns, tp_count = dims
    per_plane = rows * columns
    token_count, width = normed.shape
    padded = -(-group // 16) * 16
    slots = slot_index.reshape(token_count, TOPK).astype(jnp.float32)
    slots = jnp.concatenate([slots, route_weights], axis=1).T
    hbm = pl.BlockSpec(memory_space=pl.ANY)
    dma = pltpu.SemaphoreType.DMA
    return pl.pallas_call(
        functools.partial(dispatch_kernel, dims, group),
        out_shape=[
            jax.ShapeDtypeStruct((tp_count, planes * per_plane, padded, width), jnp.bfloat16),
            jax.ShapeDtypeStruct((planes, 2 * TOPK, token_count), jnp.float32),
        ],
        in_specs=[hbm, hbm],
        out_specs=[pl.BlockSpec(memory_space=pltpu.VMEM)] * 2,
        scratch_shapes=[
            pltpu.VMEM((planes, token_count, width), jnp.bfloat16),
            pltpu.VMEM((planes, per_plane, padded, width), jnp.bfloat16),
            dma((2,)),
            dma((planes,)),
            dma((planes,)),
            dma((planes, 2)),
            dma((planes, 2)),
            dma((planes, per_plane)),
            dma((planes, per_plane)),
            dma((planes, max(1, tp_count - 1))),
            dma((planes, max(1, tp_count - 1))),
        ],
        compiler_params=pltpu.CompilerParams(
            collective_id=1, has_side_effects=True, vmem_limit_bytes=56 * 1024 * 1024
        ),
        name="dispatch",
    )(normed, slots)


def combine_kernel(
    dims,
    group,
    parts_ref,
    marks_ref,
    out_ref,
    mine,
    theirs,
    stage,
    back,
    leaving,
    landed,
    load_sem,
    pair_recv,
    pair_send,
    cell_recv,
    cell_send,
    far_recv,
    far_send,
):
    planes, rows, columns, tp_count = dims
    per_plane = rows * columns
    plane, cell, sp, tp = plane_greeting(planes, rows, columns, tp_count)
    padded = stage.shape[2]
    token_count = out_ref.shape[0]
    order = list(range(1, planes)) + [0]

    def source_of(step):
        return (plane + step) % planes

    def load(step):
        source = source_of(step)
        return pltpu.make_async_copy(
            parts_ref.at[tp, pl.ds(source * per_plane, per_plane)],
            mine.at[source],
            load_sem.at[step],
        )

    def to_pair(step, k):
        source = source_of(step)
        other = (tp + k) % tp_count
        return pltpu.make_async_remote_copy(
            src_ref=parts_ref.at[other, pl.ds(source * per_plane, per_plane)],
            dst_ref=theirs.at[k - 1, source],
            send_sem=pair_send.at[step, k - 1],
            recv_sem=pair_recv.at[step, k - 1],
            device_id={"tp": other},
            device_id_type=MESH,
        )

    def to_cell(step, k):
        source = source_of(step)
        other = (cell + k) % per_plane
        return pltpu.make_async_remote_copy(
            src_ref=stage.at[source, other],
            dst_ref=back.at[source, cell],
            send_sem=cell_send.at[step, k],
            recv_sem=cell_recv.at[step, (per_plane - k) % per_plane],
            device_id={"sp": plane * per_plane + other},
            device_id_type=MESH,
        )

    def to_far(step):
        return pltpu.make_async_remote_copy(
            src_ref=leaving.at[step],
            dst_ref=landed.at[step],
            send_sem=far_send.at[step],
            recv_sem=far_recv.at[step],
            device_id={"sp": source_of(step) * per_plane + cell},
            device_id_type=MESH,
        )

    for step in order:
        load(step).start()
        for k in range(1, tp_count):
            to_pair(step, k).start()

    def body(step):
        source = source_of(step)
        load(step).wait()
        for k in range(1, tp_count):
            to_pair(step, k).wait_recv()
        for k in list(range(1, per_plane)) + [0]:
            other = (cell + k) % per_plane
            total = mine[source, other].astype(jnp.float32)
            for i in range(tp_count - 1):
                total += theirs[i, source, other].astype(jnp.float32)
            if k == 0:
                back[source, cell] = total.astype(jnp.bfloat16)
            else:
                stage[source, other] = total.astype(jnp.bfloat16)
        for k in range(1, per_plane):
            to_cell(step, k).start()

    def finish(step):
        source = source_of(step)
        for k in range(1, per_plane):
            pltpu.make_async_remote_copy(
                src_ref=stage.at[source, cell],
                dst_ref=back.at[source, (cell + k) % per_plane],
                send_sem=cell_send.at[step, k],
                recv_sem=cell_recv.at[step, k],
                device_id={"sp": sp},
                device_id_type=MESH,
            ).wait_recv()
        marks = marks_ref[source]
        row = lax.broadcasted_iota(jnp.int32, (per_plane * padded, token_count), 0)
        block = lax.div(row, padded)
        inner = row - block * padded
        wanted = jnp.where(
            inner < group, inner + (plane * per_plane + block) * group, -1
        ).astype(jnp.float32)
        share = jnp.zeros(wanted.shape, jnp.float32)
        for choice in range(TOPK):
            share += jnp.where(
                marks[choice : choice + 1, :] == wanted,
                marks[TOPK + choice : TOPK + choice + 1, :],
                0.0,
            )
        high = share.astype(jnp.bfloat16)
        low = (share - high.astype(jnp.float32)).astype(jnp.bfloat16)
        both = jnp.concatenate([high, low], axis=1)
        for at in range(0, out_ref.shape[1], 512):
            values = back[source, :, :, at : at + 512].reshape(per_plane * padded, 512)
            pieces = lax.dot_general(
                both, values, (((0,), (0,)), ((), ())), preferred_element_type=jnp.float32
            )
            total = pieces[:token_count] + pieces[token_count:]
            if step == 0:
                out_ref[:, at : at + 512] = total
            else:
                leaving[step, :, at : at + 512] = total.astype(jnp.bfloat16)
        if step > 0:
            to_far(step).start()

    for index, step in enumerate(order):
        body(step)
        if index > 0:
            finish(order[index - 1])
    finish(order[-1])
    for step in range(1, planes):
        to_far(step).wait_recv()
        out_ref[...] += landed[step].astype(jnp.float32)
    for step in order:
        for k in range(1, tp_count):
            to_pair(step, k).wait_send()
        for k in range(1, per_plane):
            to_cell(step, k).wait_send()
        if step > 0:
            to_far(step).wait_send()


def combined_rows(dims, group, parts, marks):
    planes, rows, columns, tp_count = dims
    per_plane = rows * columns
    padded, width = parts.shape[2:]
    token_count = marks.shape[2]
    dma = pltpu.SemaphoreType.DMA
    block = (planes, per_plane, padded, width)
    pairs = max(1, tp_count - 1)
    return pl.pallas_call(
        functools.partial(combine_kernel, dims, group),
        out_shape=jax.ShapeDtypeStruct((token_count, width), jnp.float32),
        in_specs=[pl.BlockSpec(memory_space=pl.ANY), pl.BlockSpec(memory_space=pltpu.VMEM)],
        out_specs=pl.BlockSpec(memory_space=pltpu.VMEM),
        scratch_shapes=[
            pltpu.VMEM(block, jnp.bfloat16),
            pltpu.VMEM((pairs,) + block, jnp.bfloat16),
            pltpu.VMEM(block, jnp.bfloat16),
            pltpu.VMEM(block, jnp.bfloat16),
            pltpu.VMEM((planes, token_count, width), jnp.bfloat16),
            pltpu.VMEM((planes, token_count, width), jnp.bfloat16),
            dma((planes,)),
            dma((planes, pairs)),
            dma((planes, pairs)),
            dma((planes, per_plane)),
            dma((planes, per_plane)),
            dma((planes,)),
            dma((planes,)),
        ],
        compiler_params=pltpu.CompilerParams(
            collective_id=2, has_side_effects=True, vmem_limit_bytes=56 * 1024 * 1024
        ),
        name="combine",
    )(parts, marks)


def run_experts(incoming, expert_gate, expert_up, expert_down, capacity):
    sources = incoming.shape[0]
    local_experts = expert_gate.shape[0]
    grouped = incoming.reshape(sources, local_experts, capacity, D)
    gate_part = jnp.einsum(
        "rjcd,jdf->rjcf", grouped, expert_gate, preferred_element_type=jnp.float32
    )
    up_part = jnp.einsum("rjcd,jdf->rjcf", grouped, expert_up, preferred_element_type=jnp.float32)
    hidden = (jax.nn.silu(gate_part) * up_part).astype(jnp.bfloat16)
    result = jnp.einsum("rjcf,jfd->rjcd", hidden, expert_down, preferred_element_type=jnp.float32)
    return result.reshape(sources, local_experts * capacity, D)


def shards(
    queries_narrow,
    keys_narrow,
    values_narrow,
    queries_wide,
    keys_wide,
    values_wide,
    lambda_narrow,
    lambda_wide,
    gain_narrow,
    gain_wide,
    out_narrow,
    out_wide,
    stream,
    gain_mix,
    gain_ffn,
    gain_post,
    shared_gate,
    shared_up,
    shared_down,
    expert_gate,
    expert_up,
    expert_down,
    expert_ids,
    route_weights,
):
    sp_count = lax.axis_size("sp")
    attended = attended_rows(
        sp_count,
        lax.axis_size("tp"),
        queries_narrow,
        keys_narrow,
        values_narrow,
        queries_wide,
        keys_wide,
        values_wide,
        lambda_narrow,
        lambda_wide,
        gain_narrow,
        gain_wide,
    )
    narrow_width = out_narrow.shape[0] // attended.shape[0]
    attended = attended.transpose(1, 0, 2)
    narrow_rows = attended[:, :, :narrow_width].reshape(attended.shape[0], -1)
    wide_rows = attended[:, :, narrow_width:].reshape(attended.shape[0], -1)
    projected = jnp.dot(narrow_rows, out_narrow, preferred_element_type=jnp.float32) + jnp.dot(
        wide_rows, out_wide, preferred_element_type=jnp.float32
    )
    mixed_rows = (stream.astype(jnp.float32) + rms_scale(projected, gain_mix)).astype(jnp.bfloat16)
    normed = rms_scale(mixed_rows.astype(jnp.float32), gain_ffn).astype(jnp.bfloat16)
    row_count = normed.shape[0]
    tp_count = lax.axis_size("tp")
    local_experts = expert_gate.shape[0]
    experts_all = local_experts * sp_count
    capacity = max(2, 3 * row_count * TOPK // (2 * experts_all))
    flat_ids = expert_ids.reshape(-1)
    onehot = (flat_ids[:, None] == jnp.arange(experts_all, dtype=jnp.int32)[None, :]).astype(
        jnp.int32
    )
    earlier = jnp.cumsum(onehot, axis=0) - onehot
    slot_rank = jnp.sum(earlier * onehot, axis=1)
    slot_index = flat_ids * capacity + slot_rank
    group = local_experts * capacity
    dims = plane_shape(sp_count) + (tp_count,)
    all_rows, marks = dispatched_rows(dims, group, normed, slot_index, route_weights)
    padded = all_rows.shape[2]
    partials = run_experts(
        all_rows[:, :, :group].reshape(tp_count * sp_count, group, D),
        expert_gate,
        expert_up,
        expert_down,
        capacity,
    )
    partials = partials.astype(jnp.bfloat16).reshape(tp_count, sp_count, group, D)
    if padded > group:
        partials = jnp.pad(partials, ((0, 0), (0, 0), (0, padded - group), (0, 0)))
    routed = combined_rows(dims, group, partials, marks)
    shared_hidden = (
        jax.nn.silu(jnp.dot(normed, shared_gate, preferred_element_type=jnp.float32))
        * jnp.dot(normed, shared_up, preferred_element_type=jnp.float32)
    ).astype(jnp.bfloat16)
    shared_out = jnp.dot(shared_hidden, shared_down, preferred_element_type=jnp.float32)
    combined = shared_out + routed
    return (mixed_rows.astype(jnp.float32) + rms_scale(combined, gain_post)).astype(jnp.bfloat16)


def solution(mesh):
    return jax.shard_map(
        shards,
        mesh=mesh,
        in_specs=(
            P("sp", "tp"),
            P("sp", "tp"),
            P("sp", "tp"),
            P("sp", "tp"),
            P("sp", "tp"),
            P("sp", "tp"),
            P("tp"),
            P("tp"),
            P(),
            P(),
            P(),
            P(),
            P(("sp", "tp"), None),
            P(),
            P(),
            P(),
            P(),
            P(),
            P(),
            P("sp", None, "tp"),
            P("sp", None, "tp"),
            P("sp", "tp", None),
            P(("sp", "tp"), None),
            P(("sp", "tp"), None),
        ),
        out_specs=P(("sp", "tp"), None),
        check_vma=False,
    )
```

```python
import functools
import math

import jax
import jax.numpy as jnp
from jax import lax
from jax.experimental import pallas as pl
from jax.experimental.pallas import tpu as pltpu
from jax.sharding import PartitionSpec as P

D = 2048
DN = 64
VN = 128
DW = 128
VW = 256
TOPK = 4


EPS = 1e-06


def rms_scale(values, gain_row):
    return values * lax.rsqrt(jnp.mean(values * values, axis=-1, keepdims=True) + EPS) * gain_row


MESH = pl.DeviceIdType.MESH
LOG2E = math.log2(math.e)
MASKED = -1e30


def plane_shape(sp_count):
    bits = sp_count.bit_length() - 1
    if 1 << bits != sp_count:
        return sp_count, 1, 1
    columns = 1 << (bits // 3 if bits % 3 == 0 else (bits - bits // 2) // 2)
    rows = columns
    return sp_count // (rows * columns), rows, columns


def attend_kernel(
    dims,
    qn_ref,
    kn_ref,
    vn_ref,
    qw_ref,
    kw_ref,
    vw_ref,
    lamn_ref,
    lamw_ref,
    gainn_ref,
    gainw_ref,
    out_ref,
    kv,
    att,
    row_max,
    row_sum,
    acc_n,
    acc_w,
    load_sem,
    recv_sem,
    up_sem,
    first_sem,
    second_sem,
    pair_send,
    pair_recv,
    pair_ready,
):
    planes, rows, columns, tp_count = dims
    per_plane = rows * columns
    sp = lax.axis_index("sp")
    tp = lax.axis_index("tp")
    plane = sp // per_plane
    cell = sp % per_plane
    y = cell // columns
    x = cell % columns
    queries = qn_ref.shape[2]
    half_rows = queries // 2

    own = []
    begin = 0
    for index, ref in enumerate((kn_ref, vn_ref, kw_ref, vw_ref)):
        width = ref.shape[1]
        own.append(
            pltpu.make_async_copy(ref, kv.at[0, cell, :, pl.ds(begin, width)], load_sem.at[index])
        )
        begin += width
    for copy in own:
        copy.start()

    def line(axis):
        if axis == 0:
            return [((y + k) % rows) * columns + x for k in range(1, rows)]
        return [y * columns + (x + k) % columns for k in range(1, columns)]

    def crossed(other, axis):
        oy = other // columns
        ox = other % columns
        if axis == 0:
            return [((oy + k) % rows) * columns + ox for k in range(1, rows)]
        return [oy * columns + (ox + k) % columns for k in range(1, columns)]

    barrier = pltpu.get_barrier_semaphore()
    for other in line(0) + line(1):
        pl.semaphore_signal(
            barrier, inc=1, device_id={"sp": plane * per_plane + other}, device_id_type=MESH
        )
    for k in range(1, tp_count):
        pl.semaphore_signal(
            barrier, inc=1, device_id={"tp": (tp + k) % tp_count}, device_id_type=MESH
        )

    @pl.when(plane > 0)
    def _():
        pl.semaphore_signal(barrier, inc=1, device_id={"sp": sp - per_plane}, device_id_type=MESH)

    @pl.when(plane < planes - 1)
    def _():
        pl.semaphore_signal(barrier, inc=1, device_id={"sp": sp + per_plane}, device_id_type=MESH)

    below = (plane > 0).astype(jnp.int32)
    above = (plane < planes - 1).astype(jnp.int32)
    pl.semaphore_wait(barrier, rows - 1 + columns - 1 + tp_count - 1 + below + above)

    for copy in own:
        copy.wait()

    def piece(depth, block, half):
        return kv.at[depth, block, pl.ds(half * half_rows, half_rows), :]

    def remote(depth, to_depth, block, half, target, send):
        return pltpu.make_async_remote_copy(
            src_ref=piece(depth, block, half),
            dst_ref=piece(to_depth, block, half),
            send_sem=send,
            recv_sem=recv_sem.at[to_depth, block, half],
            device_id={"sp": target},
            device_id_type=MESH,
        )

    def arrived(depth, block, half):
        pltpu.make_async_remote_copy(
            src_ref=piece(depth, block, half),
            dst_ref=piece(depth, block, half),
            send_sem=up_sem.at[0, 0],
            recv_sem=recv_sem.at[depth, block, half],
            device_id={"sp": sp},
            device_id_type=MESH,
        ).wait_recv()

    def up_copies(depth):
        return [
            remote(depth, depth + 1, cell, half, sp + per_plane, up_sem.at[depth, half])
            for half in range(2)
        ]

    def direct_copies(depth):
        copies = []
        for half in range(2):
            for k, other in enumerate(line(half)):
                copies.append(
                    remote(
                        depth,
                        depth,
                        cell,
                        half,
                        plane * per_plane + other,
                        first_sem.at[depth, half, k],
                    )
                )
            for k, other in enumerate(line(1 - half)):
                copies.append(
                    remote(
                        depth,
                        depth,
                        cell,
                        half,
                        plane * per_plane + other,
                        second_sem.at[depth, half, 0, k],
                    )
                )
        return copies

    def relay_copies(depth):
        groups = []
        for half in range(2):
            for i, block in enumerate(line(half)):
                copies = [
                    remote(
                        depth,
                        depth,
                        block,
                        half,
                        plane * per_plane + other,
                        second_sem.at[depth, half, i + 1, k],
                    )
                    for k, other in enumerate(line(1 - half))
                ]
                groups.append((block, half, copies))
        return groups

    def issue(depth):
        @pl.when(plane < planes - 1)
        def _():
            for copy in up_copies(depth):
                copy.start()

        for copy in direct_copies(depth):
            copy.start()

    def relay(depth):
        for block, half, copies in relay_copies(depth):
            arrived(depth, block, half)
            for copy in copies:
                copy.start()

    def finish(depth):
        for half in range(2):
            for block in line(1 - half):
                arrived(depth, block, half)
            for first in line(half):
                for block in crossed(first, 1 - half):
                    arrived(depth, block, half)

    row_max[...] = jnp.full_like(row_max, MASKED)
    row_sum[...] = jnp.zeros_like(row_sum)
    acc_n[...] = jnp.zeros_like(acc_n)
    acc_w[...] = jnp.zeros_like(acc_w)
    heads_n = qn_ref.shape[0]
    heads_w = qw_ref.shape[1] // kw_ref.shape[1]
    width_k = kn_ref.shape[1]
    value_n = vn_ref.shape[1]
    begin_kw = width_k + value_n
    map_w = kw_ref.shape[1] // 2
    begin_vw = begin_kw + 2 * map_w
    value_w = vw_ref.shape[1]
    chunk = math.gcd(per_plane, 4)
    key_rows = chunk * queries

    def tile(query, key, value, factor, mask, state, acc, slot):
        scores = lax.dot_general(
            query, key, (((1,), (1,)), ((), ())), preferred_element_type=jnp.float32
        )
        if mask is not None:
            scores = jnp.where(mask, scores, MASKED)
        before = row_max[state][:, :1]
        now = jnp.maximum(before, jnp.max(scores, axis=1, keepdims=True))
        weights = jnp.exp2((scores - now) * factor)
        decay = jnp.exp2((before - now) * factor)
        total = row_sum[state][:, :1] * decay + jnp.sum(weights, axis=1, keepdims=True)
        acc[slot] = acc[slot] * decay + jnp.dot(
            weights.astype(jnp.bfloat16), value, preferred_element_type=jnp.float32
        )
        row_max[state] = jnp.broadcast_to(now, row_max.shape[1:])
        row_sum[state] = jnp.broadcast_to(total, row_sum.shape[1:])

    def attend(depth, masked):
        def part(at):
            def columns_of(begin, width):
                return kv[depth, pl.ds(at, chunk), :, begin : begin + width].reshape(
                    key_rows, width
                )

            mask = None
            if masked:
                query_pos = cell * queries + lax.broadcasted_iota(
                    jnp.int32, (queries, key_rows), 0
                )
                key_pos = at * queries + lax.broadcasted_iota(jnp.int32, (queries, key_rows), 1)
                mask = key_pos <= query_pos

            def narrow(head, carry):
                key = columns_of(0, width_k)
                value = columns_of(width_k, value_n)
                for which in range(2):
                    index = head * 2 + which
                    tile(
                        qn_ref[head, which],
                        key,
                        value,
                        DN**-0.5 * LOG2E,
                        mask,
                        index,
                        acc_n,
                        index,
                    )
                return carry

            def wide(head, carry):
                value = columns_of(begin_vw, value_w)
                for which in range(2):
                    index = head * 2 + which
                    tile(
                        qw_ref[:, pl.ds(pl.multiple_of(index * map_w, map_w), map_w)],
                        columns_of(begin_kw + which * map_w, map_w),
                        value,
                        DW**-0.5 * LOG2E,
                        mask,
                        2 * heads_n + index,
                        acc_w,
                        index,
                    )
                return carry

            lax.fori_loop(0, heads_n, narrow, 0)
            lax.fori_loop(0, heads_w, wide, 0)

        if per_plane == chunk:
            part(0)
        else:

            def step(at, carry):
                part(at * chunk)
                return carry

            lax.fori_loop(0, per_plane // chunk, step, 0)

    def advance(depth):
        @pl.when(depth < plane)
        def _():
            for half in range(2):
                arrived(depth + 1, cell, half)
            issue(depth + 1)

    def relay_next(depth):
        @pl.when(depth < plane)
        def _():
            relay(depth + 1)

    issue(0)
    relay(0)
    advance(0)
    finish(0)
    attend(0, True)
    relay_next(0)

    def depth_step(depth, carry):
        advance(depth)
        finish(depth)
        attend(depth, False)
        relay_next(depth)
        return carry

    lax.fori_loop(1, plane + 1, depth_step, 0)

    def close(first, second, lam, gain):
        head = first - lam * second
        scale = lax.rsqrt(jnp.mean(head * head, axis=1, keepdims=True) + EPS)
        return (head * scale * gain).astype(jnp.bfloat16)

    for head in range(heads_n):
        maps = [acc_n[2 * head + k] / row_sum[2 * head + k][:, :1] for k in range(2)]
        att[:, head * value_n : (head + 1) * value_n] = close(
            maps[0], maps[1], lamn_ref[head], gainn_ref[...]
        )
    begin_w = heads_n * value_n
    for head in range(heads_w):
        maps = [
            acc_w[2 * head + k] / row_sum[2 * (heads_n + head) + k][:, :1] for k in range(2)
        ]
        att[:, begin_w + head * value_w : begin_w + (head + 1) * value_w] = close(
            maps[0], maps[1], lamw_ref[head], gainw_ref[...]
        )

    def drain(depth, carry):
        @pl.when(plane < planes - 1)
        def _():
            for copy in up_copies(depth):
                copy.wait_send()

        for copy in direct_copies(depth):
            copy.wait_send()
        for _block, _half, copies in relay_copies(depth):
            for copy in copies:
                copy.wait_send()
        return carry

    lax.fori_loop(0, plane + 1, drain, 0)
    for k in range(1, tp_count):
        pl.semaphore_signal(
            pair_ready, inc=1, device_id={"tp": (tp + k) % tp_count}, device_id_type=MESH
        )
    pl.semaphore_wait(pair_ready, tp_count - 1)
    share = out_ref.shape[1]
    copies = []
    for k in range(1, tp_count):
        other = (tp + k) % tp_count
        copies.append(
            pltpu.make_async_remote_copy(
                src_ref=att.at[pl.ds(pl.multiple_of(other * share, share), share), :],
                dst_ref=out_ref.at[tp],
                send_sem=pair_send.at[k - 1],
                recv_sem=pair_recv.at[k - 1],
                device_id={"tp": other},
                device_id_type=MESH,
            )
        )
    for copy in copies:
        copy.start()
    out_ref[tp] = att[pl.ds(pl.multiple_of(tp * share, share), share), :]
    for copy in copies:
        copy.wait()


def attended_rows(
    sp_count,
    tp_count,
    queries_narrow,
    keys_narrow,
    values_narrow,
    queries_wide,
    keys_wide,
    values_wide,
    lambda_narrow,
    lambda_wide,
    gain_narrow,
    gain_wide,
):
    planes, rows, columns = plane_shape(sp_count)
    count = queries_narrow.shape[0]
    heads_n = queries_narrow.shape[1] // (2 * DN)
    heads_w = queries_wide.shape[1] // (2 * DW)
    maps = queries_narrow.reshape(count, heads_n, 2, DN).transpose(1, 2, 0, 3)
    padded = jnp.stack(
        [
            jnp.pad(maps[:, 0], ((0, 0), (0, 0), (0, DN))),
            jnp.pad(maps[:, 1], ((0, 0), (0, 0), (DN, 0))),
        ],
        axis=1,
    )
    width = (
        keys_narrow.shape[1] + values_narrow.shape[1] + keys_wide.shape[1] + values_wide.shape[1]
    )
    per_plane = rows * columns
    features = heads_n * VN + heads_w * VW
    longest = max(rows, columns)
    tiles = 2 * (heads_n + heads_w)
    vmem = pl.BlockSpec(memory_space=pltpu.VMEM)
    smem = pl.BlockSpec(memory_space=pltpu.SMEM)
    hbm = pl.BlockSpec(memory_space=pl.ANY)
    return pl.pallas_call(
        functools.partial(attend_kernel, (planes, rows, columns, tp_count)),
        out_shape=jax.ShapeDtypeStruct((tp_count, count // tp_count, features), jnp.bfloat16),
        in_specs=[vmem, hbm, hbm, vmem, hbm, hbm, smem, smem, vmem, vmem],
        out_specs=vmem,
        scratch_shapes=[
            pltpu.VMEM((planes, per_plane, count, width), jnp.bfloat16),
            pltpu.VMEM((count, features), jnp.bfloat16),
            pltpu.VMEM((tiles, count, 128), jnp.float32),
            pltpu.VMEM((tiles, count, 128), jnp.float32),
            pltpu.VMEM((2 * heads_n, count, VN), jnp.float32),
            pltpu.VMEM((2 * heads_w, count, VW), jnp.float32),
            pltpu.SemaphoreType.DMA((4,)),
            pltpu.SemaphoreType.DMA((planes, per_plane, 2)),
            pltpu.SemaphoreType.DMA((planes, 2)),
            pltpu.SemaphoreType.DMA((planes, 2, longest)),
            pltpu.SemaphoreType.DMA((planes, 2, longest, longest)),
            pltpu.SemaphoreType.DMA((max(1, tp_count - 1),)),
            pltpu.SemaphoreType.DMA((max(1, tp_count - 1),)),
            pltpu.SemaphoreType.REGULAR,
        ],
        compiler_params=pltpu.CompilerParams(
            collective_id=0, has_side_effects=True, vmem_limit_bytes=56 * 1024 * 1024
        ),
        name="gather_attend",
    )(
        padded,
        keys_narrow,
        values_narrow,
        queries_wide,
        keys_wide,
        values_wide,
        lambda_narrow,
        lambda_wide,
        gain_narrow.reshape(1, -1),
        gain_wide.reshape(1, -1),
    )


def plane_greeting(planes, rows, columns, tp_count):
    per_plane = rows * columns
    sp = lax.axis_index("sp")
    tp = lax.axis_index("tp")
    plane = sp // per_plane
    cell = sp % per_plane
    barrier = pltpu.get_barrier_semaphore()
    for k in range(1, per_plane):
        pl.semaphore_signal(
            barrier,
            inc=1,
            device_id={"sp": plane * per_plane + (cell + k) % per_plane},
            device_id_type=MESH,
        )
    for k in range(1, planes):
        pl.semaphore_signal(
            barrier,
            inc=1,
            device_id={"sp": (plane + k) % planes * per_plane + cell},
            device_id_type=MESH,
        )
    for k in range(1, tp_count):
        pl.semaphore_signal(
            barrier, inc=1, device_id={"tp": (tp + k) % tp_count}, device_id_type=MESH
        )
    pl.semaphore_wait(barrier, per_plane - 1 + planes - 1 + tp_count - 1)
    return plane, cell, sp, tp


def dispatch_kernel(
    dims,
    group,
    normed_ref,
    slots_ref,
    inbox,
    marks,
    held,
    stage,
    load_sem,
    row_recv,
    mark_recv,
    row_send,
    mark_send,
    cell_recv,
    cell_send,
    pair_recv,
    pair_send,
):
    planes, rows, columns, tp_count = dims
    per_plane = rows * columns
    sp_now = lax.axis_index("sp")
    mine = sp_now // per_plane
    loads = [
        pltpu.make_async_copy(normed_ref, held.at[mine], load_sem.at[0]),
        pltpu.make_async_copy(slots_ref, marks.at[mine], load_sem.at[1]),
    ]
    for copy in loads:
        copy.start()
    plane, cell, sp, tp = plane_greeting(planes, rows, columns, tp_count)
    for copy in loads:
        copy.wait()
    padded = stage.shape[2]
    token_count = held.shape[1]

    def hops(source, way):
        target = {"sp": (sp + per_plane * (1 if way == 0 else planes - 1)) % (planes * per_plane)}
        return [
            pltpu.make_async_remote_copy(
                src_ref=marks.at[source],
                dst_ref=marks.at[source],
                send_sem=mark_send.at[source, way],
                recv_sem=mark_recv.at[source],
                device_id=target,
                device_id_type=MESH,
            ),
            pltpu.make_async_remote_copy(
                src_ref=held.at[source],
                dst_ref=held.at[source],
                send_sem=row_send.at[source, way],
                recv_sem=row_recv.at[source],
                device_id=target,
                device_id_type=MESH,
            ),
        ]

    def to_cell(source, k):
        other = (cell + k) % per_plane
        return pltpu.make_async_remote_copy(
            src_ref=stage.at[source, other],
            dst_ref=inbox.at[tp, source * per_plane + cell],
            send_sem=cell_send.at[source, k],
            recv_sem=cell_recv.at[source, (per_plane - k) % per_plane],
            device_id={"sp": plane * per_plane + other},
            device_id_type=MESH,
        )

    def to_pair(source, k):
        block = inbox.at[tp, pl.ds(source * per_plane, per_plane)]
        return pltpu.make_async_remote_copy(
            src_ref=block,
            dst_ref=block,
            send_sem=pair_send.at[source, k - 1],
            recv_sem=pair_recv.at[source, k - 1],
            device_id={"tp": (tp + k) % tp_count},
            device_id_type=MESH,
        )

    steps = [(0, 0)] + [(d, way) for d in range(1, planes) for way in range(2)]

    def of_step(d, way):
        source = plane - d if way == 0 else plane + d
        exists = source >= 0 if way == 0 else source < planes
        return source, exists

    def onward(source, d, way, act):
        for side in ((0, 1) if d == 0 else (way,)):

            @pl.when(plane < planes - 1 if side == 0 else plane > 0)
            def _(side=side):
                for copy in hops(source, side):
                    act(copy)

    def start(copy):
        copy.start()

    def wait_send(copy):
        copy.wait_send()

    def body(d, way):
        source, exists = of_step(d, way)

        @pl.when(exists)
        def _():
            if d > 0:
                for copy in hops(source, way):
                    copy.wait_recv()
            onward(source, d, way, start)
            tokens = held[source]
            slots = marks[source]
            row = lax.broadcasted_iota(jnp.int32, (padded, token_count), 0)
            for k in list(range(1, per_plane)) + [0]:
                other = (cell + k) % per_plane
                base = (plane * per_plane + other) * group
                wanted = jnp.where(row < group, row + base, -1).astype(jnp.float32)
                hit = slots[0:1, :] == wanted
                for choice in range(1, TOPK):
                    hit = hit | (slots[choice : choice + 1, :] == wanted)
                chosen = jnp.dot(
                    jnp.where(hit, 1.0, 0.0).astype(jnp.bfloat16),
                    tokens,
                    preferred_element_type=jnp.float32,
                ).astype(jnp.bfloat16)
                if k == 0:
                    inbox[tp, source * per_plane + cell] = chosen
                else:
                    stage[source, other] = chosen
            for k in range(1, per_plane):
                to_cell(source, k).start()

    def finish(d, way):
        source, exists = of_step(d, way)

        @pl.when(exists)
        def _():
            for k in range(1, per_plane):
                pltpu.make_async_remote_copy(
                    src_ref=stage.at[source, cell],
                    dst_ref=inbox.at[tp, source * per_plane + (cell + k) % per_plane],
                    send_sem=cell_send.at[source, k],
                    recv_sem=cell_recv.at[source, k],
                    device_id={"sp": sp},
                    device_id_type=MESH,
                ).wait_recv()
            for k in range(1, tp_count):
                to_pair(source, k).start()

    for index, step in enumerate(steps):
        body(*step)
        if index > 0:
            finish(*steps[index - 1])
    finish(*steps[-1])
    for d, way in steps:
        source, exists = of_step(d, way)

        @pl.when(exists)
        def _(source=source, d=d, way=way):
            onward(source, d, way, wait_send)
            for k in range(1, per_plane):
                to_cell(source, k).wait_send()
            for k in range(1, tp_count):
                to_pair(source, k).wait()


def dispatched_rows(dims, group, normed, slot_index, route_weights):
    planes, rows, columns, tp_count = dims
    per_plane = rows * columns
    token_count, width = normed.shape
    padded = -(-group // 16) * 16
    slots = slot_index.reshape(token_count, TOPK).astype(jnp.float32)
    slots = jnp.concatenate([slots, route_weights], axis=1).T
    hbm = pl.BlockSpec(memory_space=pl.ANY)
    dma = pltpu.SemaphoreType.DMA
    return pl.pallas_call(
        functools.partial(dispatch_kernel, dims, group),
        out_shape=[
            jax.ShapeDtypeStruct((tp_count, planes * per_plane, padded, width), jnp.bfloat16),
            jax.ShapeDtypeStruct((planes, 2 * TOPK, token_count), jnp.float32),
        ],
        in_specs=[hbm, hbm],
        out_specs=[pl.BlockSpec(memory_space=pltpu.VMEM)] * 2,
        scratch_shapes=[
            pltpu.VMEM((planes, token_count, width), jnp.bfloat16),
            pltpu.VMEM((planes, per_plane, padded, width), jnp.bfloat16),
            dma((2,)),
            dma((planes,)),
            dma((planes,)),
            dma((planes, 2)),
            dma((planes, 2)),
            dma((planes, per_plane)),
            dma((planes, per_plane)),
            dma((planes, max(1, tp_count - 1))),
            dma((planes, max(1, tp_count - 1))),
        ],
        compiler_params=pltpu.CompilerParams(
            collective_id=1, has_side_effects=True, vmem_limit_bytes=56 * 1024 * 1024
        ),
        name="dispatch",
    )(normed, slots)


def combine_kernel(
    dims,
    group,
    parts_ref,
    marks_ref,
    out_ref,
    mine,
    theirs,
    stage,
    back,
    leaving,
    landed,
    load_sem,
    pair_recv,
    pair_send,
    cell_recv,
    cell_send,
    far_recv,
    far_send,
):
    planes, rows, columns, tp_count = dims
    per_plane = rows * columns
    plane, cell, sp, tp = plane_greeting(planes, rows, columns, tp_count)
    padded = stage.shape[2]
    token_count = out_ref.shape[0]
    order = list(range(1, planes)) + [0]

    def source_of(step):
        return (plane + step) % planes

    def load(step):
        source = source_of(step)
        return pltpu.make_async_copy(
            parts_ref.at[tp, pl.ds(source * per_plane, per_plane)],
            mine.at[source],
            load_sem.at[step],
        )

    def to_pair(step, k):
        source = source_of(step)
        other = (tp + k) % tp_count
        return pltpu.make_async_remote_copy(
            src_ref=parts_ref.at[other, pl.ds(source * per_plane, per_plane)],
            dst_ref=theirs.at[k - 1, source],
            send_sem=pair_send.at[step, k - 1],
            recv_sem=pair_recv.at[step, k - 1],
            device_id={"tp": other},
            device_id_type=MESH,
        )

    def to_cell(step, k):
        source = source_of(step)
        other = (cell + k) % per_plane
        return pltpu.make_async_remote_copy(
            src_ref=stage.at[source, other],
            dst_ref=back.at[source, cell],
            send_sem=cell_send.at[step, k],
            recv_sem=cell_recv.at[step, (per_plane - k) % per_plane],
            device_id={"sp": plane * per_plane + other},
            device_id_type=MESH,
        )

    def to_far(step):
        return pltpu.make_async_remote_copy(
            src_ref=leaving.at[step],
            dst_ref=landed.at[step],
            send_sem=far_send.at[step],
            recv_sem=far_recv.at[step],
            device_id={"sp": source_of(step) * per_plane + cell},
            device_id_type=MESH,
        )

    for step in order:
        load(step).start()
        for k in range(1, tp_count):
            to_pair(step, k).start()

    def body(step):
        source = source_of(step)
        load(step).wait()
        for k in range(1, tp_count):
            to_pair(step, k).wait_recv()
        for k in list(range(1, per_plane)) + [0]:
            other = (cell + k) % per_plane
            total = mine[source, other].astype(jnp.float32)
            for i in range(tp_count - 1):
                total += theirs[i, source, other].astype(jnp.float32)
            if k == 0:
                back[source, cell] = total.astype(jnp.bfloat16)
            else:
                stage[source, other] = total.astype(jnp.bfloat16)
        for k in range(1, per_plane):
            to_cell(step, k).start()

    def finish(step):
        source = source_of(step)
        for k in range(1, per_plane):
            pltpu.make_async_remote_copy(
                src_ref=stage.at[source, cell],
                dst_ref=back.at[source, (cell + k) % per_plane],
                send_sem=cell_send.at[step, k],
                recv_sem=cell_recv.at[step, k],
                device_id={"sp": sp},
                device_id_type=MESH,
            ).wait_recv()
        marks = marks_ref[source]
        row = lax.broadcasted_iota(jnp.int32, (per_plane * padded, token_count), 0)
        block = lax.div(row, padded)
        inner = row - block * padded
        wanted = jnp.where(
            inner < group, inner + (plane * per_plane + block) * group, -1
        ).astype(jnp.float32)
        share = jnp.zeros(wanted.shape, jnp.float32)
        for choice in range(TOPK):
            share += jnp.where(
                marks[choice : choice + 1, :] == wanted,
                marks[TOPK + choice : TOPK + choice + 1, :],
                0.0,
            )
        high = share.astype(jnp.bfloat16)
        low = (share - high.astype(jnp.float32)).astype(jnp.bfloat16)
        both = jnp.concatenate([high, low], axis=1)
        for at in range(0, out_ref.shape[1], 512):
            values = back[source, :, :, at : at + 512].reshape(per_plane * padded, 512)
            pieces = lax.dot_general(
                both, values, (((0,), (0,)), ((), ())), preferred_element_type=jnp.float32
            )
            total = pieces[:token_count] + pieces[token_count:]
            if step == 0:
                out_ref[:, at : at + 512] = total
            else:
                leaving[step, :, at : at + 512] = total.astype(jnp.bfloat16)
        if step > 0:
            to_far(step).start()

    for index, step in enumerate(order):
        body(step)
        if index > 0:
            finish(order[index - 1])
    finish(order[-1])
    for step in range(1, planes):
        to_far(step).wait_recv()
        out_ref[...] += landed[step].astype(jnp.float32)
    for step in order:
        for k in range(1, tp_count):
            to_pair(step, k).wait_send()
        for k in range(1, per_plane):
            to_cell(step, k).wait_send()
        if step > 0:
            to_far(step).wait_send()


def combined_rows(dims, group, parts, marks):
    planes, rows, columns, tp_count = dims
    per_plane = rows * columns
    padded, width = parts.shape[2:]
    token_count = marks.shape[2]
    dma = pltpu.SemaphoreType.DMA
    block = (planes, per_plane, padded, width)
    pairs = max(1, tp_count - 1)
    return pl.pallas_call(
        functools.partial(combine_kernel, dims, group),
        out_shape=jax.ShapeDtypeStruct((token_count, width), jnp.float32),
        in_specs=[pl.BlockSpec(memory_space=pl.ANY), pl.BlockSpec(memory_space=pltpu.VMEM)],
        out_specs=pl.BlockSpec(memory_space=pltpu.VMEM),
        scratch_shapes=[
            pltpu.VMEM(block, jnp.bfloat16),
            pltpu.VMEM((pairs,) + block, jnp.bfloat16),
            pltpu.VMEM(block, jnp.bfloat16),
            pltpu.VMEM(block, jnp.bfloat16),
            pltpu.VMEM((planes, token_count, width), jnp.bfloat16),
            pltpu.VMEM((planes, token_count, width), jnp.bfloat16),
            dma((planes,)),
            dma((planes, pairs)),
            dma((planes, pairs)),
            dma((planes, per_plane)),
            dma((planes, per_plane)),
            dma((planes,)),
            dma((planes,)),
        ],
        compiler_params=pltpu.CompilerParams(
            collective_id=2, has_side_effects=True, vmem_limit_bytes=56 * 1024 * 1024
        ),
        name="combine",
    )(parts, marks)


def run_experts(incoming, expert_gate, expert_up, expert_down, capacity):
    sources = incoming.shape[0]
    local_experts = expert_gate.shape[0]
    grouped = incoming.reshape(sources, local_experts, capacity, D)
    gate_part = jnp.einsum(
        "rjcd,jdf->rjcf", grouped, expert_gate, preferred_element_type=jnp.float32
    )
    up_part = jnp.einsum("rjcd,jdf->rjcf", grouped, expert_up, preferred_element_type=jnp.float32)
    hidden = (jax.nn.silu(gate_part) * up_part).astype(jnp.bfloat16)
    result = jnp.stack(
        [
            jnp.einsum(
                "rcf,fd->rcd", hidden[:, j], expert_down[j], preferred_element_type=jnp.float32
            ).astype(jnp.bfloat16)
            for j in range(local_experts)
        ],
        axis=1,
    )
    return result.reshape(sources, local_experts * capacity, D)


def shards(
    queries_narrow,
    keys_narrow,
    values_narrow,
    queries_wide,
    keys_wide,
    values_wide,
    lambda_narrow,
    lambda_wide,
    gain_narrow,
    gain_wide,
    out_narrow,
    out_wide,
    stream,
    gain_mix,
    gain_ffn,
    gain_post,
    shared_gate,
    shared_up,
    shared_down,
    expert_gate,
    expert_up,
    expert_down,
    expert_ids,
    route_weights,
):
    sp_count = lax.axis_size("sp")
    attended = attended_rows(
        sp_count,
        lax.axis_size("tp"),
        queries_narrow,
        keys_narrow,
        values_narrow,
        queries_wide,
        keys_wide,
        values_wide,
        lambda_narrow,
        lambda_wide,
        gain_narrow,
        gain_wide,
    )
    narrow_width = out_narrow.shape[0] // attended.shape[0]
    attended = attended.transpose(1, 0, 2)
    narrow_rows = attended[:, :, :narrow_width].reshape(attended.shape[0], -1)
    wide_rows = attended[:, :, narrow_width:].reshape(attended.shape[0], -1)
    projected = jnp.dot(narrow_rows, out_narrow, preferred_element_type=jnp.float32) + jnp.dot(
        wide_rows, out_wide, preferred_element_type=jnp.float32
    )
    mixed_rows = (stream.astype(jnp.float32) + rms_scale(projected, gain_mix)).astype(jnp.bfloat16)
    normed = rms_scale(mixed_rows.astype(jnp.float32), gain_ffn).astype(jnp.bfloat16)
    row_count = normed.shape[0]
    tp_count = lax.axis_size("tp")
    local_experts = expert_gate.shape[0]
    experts_all = local_experts * sp_count
    capacity = max(2, 3 * row_count * TOPK // (2 * experts_all))
    flat_ids = expert_ids.reshape(-1)
    onehot = (flat_ids[:, None] == jnp.arange(experts_all, dtype=jnp.int32)[None, :]).astype(
        jnp.int32
    )
    earlier = jnp.cumsum(onehot, axis=0) - onehot
    slot_rank = jnp.sum(earlier * onehot, axis=1)
    slot_index = flat_ids * capacity + slot_rank
    group = local_experts * capacity
    dims = plane_shape(sp_count) + (tp_count,)
    all_rows, marks = dispatched_rows(dims, group, normed, slot_index, route_weights)
    padded = all_rows.shape[2]
    partials = run_experts(
        all_rows[:, :, :group].reshape(tp_count * sp_count, group, D),
        expert_gate,
        expert_up,
        expert_down,
        capacity,
    )
    partials = partials.astype(jnp.bfloat16).reshape(tp_count, sp_count, group, D)
    if padded > group:
        partials = jnp.pad(partials, ((0, 0), (0, 0), (0, padded - group), (0, 0)))
    routed = combined_rows(dims, group, partials, marks)
    shared_hidden = (
        jax.nn.silu(jnp.dot(normed, shared_gate, preferred_element_type=jnp.float32))
        * jnp.dot(normed, shared_up, preferred_element_type=jnp.float32)
    ).astype(jnp.bfloat16)
    shared_out = jnp.dot(shared_hidden, shared_down, preferred_element_type=jnp.float32)
    combined = shared_out + routed
    return (mixed_rows.astype(jnp.float32) + rms_scale(combined, gain_post)).astype(jnp.bfloat16)


def solution(mesh):
    return jax.shard_map(
        shards,
        mesh=mesh,
        in_specs=(
            P("sp", "tp"),
            P("sp", "tp"),
            P("sp", "tp"),
            P("sp", "tp"),
            P("sp", "tp"),
            P("sp", "tp"),
            P("tp"),
            P("tp"),
            P(),
            P(),
            P(),
            P(),
            P(("sp", "tp"), None),
            P(),
            P(),
            P(),
            P(),
            P(),
            P(),
            P("sp", None, "tp"),
            P("sp", None, "tp"),
            P("sp", "tp", None),
            P(("sp", "tp"), None),
            P(("sp", "tp"), None),
        ),
        out_specs=P(("sp", "tp"), None),
        check_vma=False,
    )
```
